32 devices in a mesh: grp: 2 (over y), ep: 8 (over z, x), tp: 2 (over core).
Axes of the slice: x: 2, y: 2, z: 4, core: 2. Of those that a mesh axis runs over, the one named last changes fastest.
Arguments:
- tokens: bfloat16 [256, 1024], P(('grp', 'ep')), parts along dimension 0, may hold values from -6 to 6
- query_weight: bfloat16 [1024, 512], P(None, 'tp'), may hold values from -0.1875 to 0.1875
- key_weight: bfloat16 [1024, 512], P(None, 'tp'), may hold values from -0.1875 to 0.1875
- value_weight: bfloat16 [1024, 512], P(None, 'tp'), may hold values from -0.1875 to 0.1875
- outgate_weight: bfloat16 [1024, 512], P(None, 'tp'), may hold values from -0.1875 to 0.1875
- ingate_weight: bfloat16 [1024, 4], P(None, 'tp'), may hold values from -0.1875 to 0.1875
- forget_weight: bfloat16 [1024, 4], P(None, 'tp'), may hold values from -0.1875 to 0.1875
- forget_bias: float32 [4], P('tp'), may hold values from -2 to 5
- head_gain: float32 [4, 128], P('tp'), may hold values from 0.1 to 1.9
- merge_weight: bfloat16 [512, 1024], P('tp'), may hold values from -0.25 to 0.25
- mixer_gain: float32 [1024], replicated, may hold values from 0.1 to 1.9
- feed_gain: float32 [1024], replicated, may hold values from 0.1 to 1.9
- memory_matrix: float32 [256, 4, 128, 128], P(('grp', 'ep'), 'tp'), parts along dimension 0, may hold values from -0.6 to 0.6
- memory_norm: float32 [256, 4, 128], P(('grp', 'ep'), 'tp'), parts along dimension 0, may hold values from -0.6 to 0.6
- memory_max: float32 [256, 4], P(('grp', 'ep'), 'tp'), parts along dimension 0, may hold values from -4 to 4
- routes: int32 [256, 2], P(('grp', 'ep')), parts along dimension 0, may hold values from 0 to 7, all different within a row; in each aligned block of 16 rows (0 to 15, 16 to 31, ...) at most 6 rows name the same one
- route_scores: bfloat16 [256, 2], P(('grp', 'ep')), parts along dimension 0, may hold values from -4 to 4
- expert_gate: bfloat16 [8, 1024, 1792], P('ep', None, 'tp'), may hold values from -0.1875 to 0.1875
- expert_up: bfloat16 [8, 1024, 1792], P('ep', None, 'tp'), may hold values from -0.1875 to 0.1875
- expert_down: bfloat16 [8, 1792, 1024], P('ep', 'tp'), may hold values from -0.125 to 0.125
- dense_left: bfloat16 [1024, 2816], P(None, 'ep'), may hold values from -0.1875 to 0.1875
- dense_right: bfloat16 [1024, 2816], P(None, 'ep'), may hold values from -0.1875 to 0.1875
- dense_down: bfloat16 [2816, 1024], P('ep'), may hold values from -0.109375 to 0.109375
- blend_weight: float32 [1024], replicated, may hold values from -0.1875 to 0.1875
Outputs:
- layer_out: bfloat16 [256, 1024], P(('grp', 'ep', 'tp')), parts along dimension 0
- new_matrix: float32 [256, 4, 128, 128], P(('grp', 'ep'), 'tp'), parts along dimension 0
- new_norm: float32 [256, 4, 128], P(('grp', 'ep'), 'tp'), parts along dimension 0
- new_max: float32 [256, 4], P(('grp', 'ep'), 'tp'), parts along dimension 0
The draws below stay inside these ranges and needn't reach their ends.
There are 2 independent parts, one for each index of `grp`. The reference program is written for one: setup_inputs(seed, part) draws one part's arguments, and reference() takes and returns one part's arrays. A program takes and returns all parts, laid end to end along the dimension named above; an argument that names none is the same for every part. Nothing has to cross between parts.
Inputs may be any that keep to these rules, and one draw needn't show every extreme that they name: `routes`: each row names 2 different experts. Among the rows of one device (aligned blocks of 16 rows) no expert is named more than 6 times, and in every draw some expert is named exactly 6 times in some block.
All inputs are finite; a program needn't handle non-finite values.
Results may differ from the reference program's by a relative error of at most 0.014.
Values may be sent and summed in bfloat16 or wider, within the bound.
A program may use at most 64 MiB of HBM per device.

```python
import math
import jax
import jax.numpy as jnp
import numpy as np
from jax import lax

D = 1024
HEADS = 4
DH = 128
MW = 512
FFE = 1792
FFD = 2816
TOP = 2
SEQ_DEV = 16
EXPERTS = 8
TOKENS = 128
CAP = 6
N_EP = 8
N_TP = 2


def block_scale(key, dims, split, low, largest):
    factor_of, own = 1.0, jax.random.fold_in(key, 6)
    for axis_at, blocks in split:
        heights = jnp.exp(jax.random.uniform(jax.random.fold_in(own, axis_at), (blocks,), jnp.float32, low / len(split), largest / len(split)))
        factor_of = factor_of * jnp.repeat(heights, dims[axis_at] // blocks).reshape([-1 if axis == axis_at else 1 for axis in range(len(dims))])
    return factor_of


def deal_out(own_key, own, number, rows, amount, top, limit, skew):
    sequence = jax.random.permutation(own_key, amount)
    packed, ordinary = portions_of(amount, rows * top, limit, skew, True), portions_of(amount, rows * top, limit, skew, False)
    places = jnp.arange(amount)

    def named(tallies, turn):
        used = int((tallies > 0).sum())
        fixed = max(1, used // 4)
        moved = fixed + (places - fixed + turn * (used - fixed)) % max(1, amount - fixed)
        return jnp.zeros((amount,), jnp.int32).at[sequence[jnp.where(places < fixed, places, moved)]].set(jnp.asarray(tallies, jnp.int32))

    tallies = jnp.where(number % 4 == 0, named(packed, number // 4), named(ordinary, number - number // 4 - 1))
    mixed = jax.random.permutation(jax.random.fold_in(own, 3), amount)
    giver, taker = mixed[0:amount // 2 * 2:2], mixed[1:amount // 2 * 2:2]
    room = jnp.minimum(tallies[giver] - 1, limit - tallies[taker]) // 2
    room = jnp.where((giver == sequence[0]) | (taker == sequence[0]) | (tallies[taker] == 0), 0, jnp.maximum(room, 0))
    moved = jax.random.randint(jax.random.fold_in(own, 4), (amount // 2,), 0, 1 << 20) % (room + 1)
    tallies = tallies.at[giver].add(-moved).at[taker].add(moved)
    members = jnp.searchsorted(jnp.cumsum(tallies), jnp.arange(rows * top), side="right").astype(jnp.int32)
    table = members.reshape(top, rows).T
    table = table[jax.random.permutation(jax.random.fold_in(own, 1), rows)]
    turn = jax.random.randint(jax.random.fold_in(own, 2), (rows, 1), 0, top)
    return jnp.take_along_axis(table, (jnp.arange(top)[None, :] + turn) % top, axis=1)


def portions_of(amount, total, reach, skew, full):
    weights = [(1 << 20) // math.isqrt(standing ** skew) + 1 for standing in range(1, amount + 1)]
    largest = reach if full else min(reach, max(-(-total // amount), total * weights[0] // sum(weights)))
    least = 1 if total - largest >= amount - 1 else 0
    given, rest = [largest] + [least] * (amount - 1), total - largest - least * (amount - 1)
    while rest > 0:
        movable = [i for i in range(1, amount) if given[i] < largest] or [i for i in range(1, amount) if given[i] < reach]
        mass, left = sum([weights[i] for i in movable]), rest
        for i in movable:
            more = min(reach - given[i], max(1, left * weights[i] // mass), rest)
            given[i] = given[i] + more
            rest = rest - more
    return np.array(given)


def centred(own_key, dims, spread, limit, pieces=(), kind=jnp.bfloat16):
    entries = jax.random.normal(own_key, dims, jnp.float32) * spread
    if len(pieces) > 0:
        entries = block_scale(own_key, dims, pieces, -0.22, 0.18) * entries
    return jnp.clip(entries, min=-limit, max=limit).astype(kind)


def setup_inputs(seed: int = 0, part: int = 0) -> dict:
    splits = jax.random.split(jax.random.key(seed), 25)
    own_keys = jax.random.split(jax.random.fold_in(splits[24], part), 25)
    tokens = centred(own_keys[0], (TOKENS, D), 1.0, 6.0, ((0, 8),))
    query_weight = centred(splits[1], (D, MW), D ** -0.5, 0.1875, ((1, 2),))
    key_weight = centred(splits[2], (D, MW), D ** -0.5, 0.1875, ((1, 2),))
    value_weight = centred(splits[3], (D, MW), D ** -0.5, 0.1875, ((1, 2),))
    outgate_weight = centred(splits[4], (D, MW), D ** -0.5, 0.1875, ((1, 2),))
    ingate_weight = centred(splits[5], (D, HEADS), D ** -0.5, 0.1875, ((1, 2),))
    forget_weight = centred(splits[6], (D, HEADS), D ** -0.5, 0.1875, ((1, 2),))
    forget_bias = jnp.clip(-2.0 + 7.0 * jax.random.uniform(splits[7], (HEADS,), jnp.float32) ** block_scale(splits[7], (HEADS,), ((0, 2),), -0.2, 0.2), -2.0, 5.0)
    head_gain = jnp.clip(1.0 + 0.18 * jax.random.normal(splits[8], (HEADS, DH), jnp.float32), 0.1, 1.9)
    merge_weight = centred(splits[9], (MW, D), MW ** -0.5, 0.25, ((0, 2),))
    mixer_gain = jnp.clip(1.0 + 0.18 * jax.random.normal(splits[10], (D,), jnp.float32), 0.1, 1.9)
    feed_gain = jnp.clip(1.0 + 0.18 * jax.random.normal(splits[11], (D,), jnp.float32), 0.1, 1.9)
    memory_matrix = centred(own_keys[12], (TOKENS, HEADS, DH, DH), 0.1, 0.6, ((0, 8), (1, 2)), jnp.float32)
    memory_norm = centred(own_keys[13], (TOKENS, HEADS, DH), 0.1, 0.6, ((0, 8), (1, 2)), jnp.float32)
    memory_max = centred(own_keys[14], (TOKENS, HEADS), 1.0, 4.0, ((0, 8), (1, 2)), jnp.float32)
    routes_keys = jax.random.split(jax.random.fold_in(own_keys[15], 1), TOKENS // SEQ_DEV)
    routes_turns = jax.random.permutation(jax.random.fold_in(own_keys[15], 3), TOKENS // SEQ_DEV)
    routes = jax.vmap(lambda own, number: deal_out(jax.random.fold_in(own_keys[15], 2), own, number, SEQ_DEV, EXPERTS, TOP, CAP, 2))(routes_keys, routes_turns).reshape((TOKENS, TOP))
    route_scores = centred(own_keys[16], (TOKENS, TOP), 1.0, 4.0, ((0, 8),))
    expert_gate = centred(splits[17], (EXPERTS, D, FFE), D ** -0.5, 0.1875, ((0, 8), (2, 2)))
    expert_up = centred(splits[18], (EXPERTS, D, FFE), D ** -0.5, 0.1875, ((0, 8), (2, 2)))
    expert_down = centred(splits[19], (EXPERTS, FFE, D), FFE ** -0.5, 0.125, ((0, 8), (1, 2)))
    dense_left = centred(splits[20], (D, FFD), D ** -0.5, 0.1875, ((1, 8),))
    dense_right = centred(splits[21], (D, FFD), D ** -0.5, 0.1875, ((1, 8),))
    dense_down = centred(splits[22], (FFD, D), FFD ** -0.5, 0.109375, ((0, 8),))
    blend_weight = centred(splits[23], (D,), D ** -0.5, 0.1875, (), jnp.float32)
    return {"tokens": tokens, "query_weight": query_weight, "key_weight": key_weight, "value_weight": value_weight, "outgate_weight": outgate_weight, "ingate_weight": ingate_weight, "forget_weight": forget_weight, "forget_bias": forget_bias, "head_gain": head_gain, "merge_weight": merge_weight, "mixer_gain": mixer_gain, "feed_gain": feed_gain, "memory_matrix": memory_matrix, "memory_norm": memory_norm, "memory_max": memory_max, "routes": routes, "route_scores": route_scores, "expert_gate": expert_gate, "expert_up": expert_up, "expert_down": expert_down, "dense_left": dense_left, "dense_right": dense_right, "dense_down": dense_down, "blend_weight": blend_weight}


epsilon = 1e-06

def rms_norm(values, gains):
    floats = values.astype(jnp.float32)
    scaled = floats * lax.rsqrt(lax.optimization_barrier(jnp.mean(floats * floats, axis=-1, keepdims=True)) + epsilon)
    return (scaled * gains).astype(jnp.bfloat16)

def memory_step(query_rows, key_rows, value_rows, in_gate, forget_pre, matrix, norm_vec, old_max):
    log_forget = jax.nn.log_sigmoid(forget_pre)
    new_max = jnp.maximum(log_forget + old_max, in_gate)
    keep = jnp.exp(log_forget + old_max - new_max)
    write = jnp.exp(in_gate - new_max)
    matrix = keep[..., None, None] * matrix + write[..., None, None] * key_rows[..., :, None] * value_rows[..., None, :]
    norm_vec = keep[..., None] * norm_vec + write[..., None] * key_rows
    numer = jnp.einsum('bhd,bhde->bhe', query_rows, matrix, precision=lax.Precision.HIGHEST)
    denom = lax.optimization_barrier(jnp.sum(query_rows * norm_vec, axis=-1))
    readout = numer / jnp.maximum(jnp.abs(denom), jnp.exp(-new_max))[..., None]
    return (readout, matrix, norm_vec, new_max)

def halves_sum(hidden, down, parts):
    width = hidden.shape[1] // parts
    total = jnp.zeros((hidden.shape[0], down.shape[1]), jnp.float32)
    for index in range(parts):
        piece = jnp.dot(hidden[:, index * width:(index + 1) * width], down[index * width:(index + 1) * width], preferred_element_type=jnp.float32).astype(jnp.bfloat16)
        piece = lax.optimization_barrier(piece)
        total = total + piece.astype(jnp.float32)
    return total

def reference(tokens, query_weight, key_weight, value_weight, outgate_weight, ingate_weight, forget_weight, forget_bias, head_gain, merge_weight, mixer_gain, feed_gain, memory_matrix, memory_norm, memory_max, routes, route_scores, expert_gate, expert_up, expert_down, dense_left, dense_right, dense_down, blend_weight):
    rows_all = tokens.shape[0]
    normed = rms_norm(tokens, mixer_gain)

    def project(weight):
        return jnp.dot(normed, weight, preferred_element_type=jnp.float32)
    query = project(query_weight).reshape(rows_all, HEADS, DH)
    key_rows = project(key_weight).reshape(rows_all, HEADS, DH) * DH ** (-0.5)
    value_rows = project(value_weight).reshape(rows_all, HEADS, DH)
    outgate_rows = project(outgate_weight).reshape(rows_all, HEADS, DH)
    in_gate = project(ingate_weight)
    forget_pre = project(forget_weight) + forget_bias
    readout, matrix, norm_vec, new_max = memory_step(query, key_rows, value_rows, in_gate, forget_pre, memory_matrix, memory_norm, memory_max)
    head_scale = lax.rsqrt(lax.optimization_barrier(jnp.mean(readout * readout, axis=(1, 2))) + epsilon)
    gated = (readout * head_gain * jax.nn.sigmoid(outgate_rows)).reshape(rows_all, MW).astype(jnp.bfloat16)
    head_total = jnp.dot(gated, merge_weight, preferred_element_type=jnp.float32)
    resid = (tokens.astype(jnp.float32) + head_scale[:, None] * head_total).astype(jnp.bfloat16)
    normed2 = rms_norm(resid, feed_gain)
    assign = SEQ_DEV * TOP
    routes_block = routes.reshape(N_EP, assign)
    member = (routes_block[..., None] == jnp.arange(EXPERTS, dtype=jnp.int32)).astype(jnp.int32)
    slot_rank = lax.optimization_barrier(jnp.sum(member * (jnp.cumsum(member, axis=1) - member), axis=-1)).astype(jnp.int32)
    source_ids = jnp.broadcast_to(jnp.arange(N_EP, dtype=jnp.int32)[:, None], (N_EP, assign))
    spread_rows = jnp.repeat(normed2, TOP, axis=0).reshape(N_EP, assign, D)
    inbox = jnp.zeros((EXPERTS, N_EP, CAP, D), jnp.bfloat16).at[routes_block, source_ids, slot_rank].set(spread_rows)

    def run_expert(operands):
        box, gate_w, up_w, down_w = operands
        rows = box.reshape(N_EP * CAP, D)
        gate_val = jnp.dot(rows, gate_w, preferred_element_type=jnp.float32)
        up_val = jnp.dot(rows, up_w, preferred_element_type=jnp.float32)
        hidden = (jax.nn.silu(gate_val) * up_val).astype(jnp.bfloat16)
        total = halves_sum(hidden, down_w, N_TP)
        return total.astype(jnp.bfloat16).reshape(N_EP, CAP, D)
    outbox = lax.map(run_expert, (inbox, expert_gate, expert_up, expert_down))
    picked = outbox[routes_block, source_ids, slot_rank].reshape(rows_all, TOP, D).astype(jnp.float32)
    route_weight = jax.nn.softmax(route_scores.astype(jnp.float32), axis=-1)
    routed = lax.optimization_barrier(jnp.sum(route_weight[..., None] * picked, axis=1))
    left_val = jnp.dot(normed2, dense_left, preferred_element_type=jnp.float32)
    right_val = jnp.dot(normed2, dense_right, preferred_element_type=jnp.float32)
    dense_hidden = (jax.nn.silu(left_val) * right_val).astype(jnp.bfloat16)
    dense = jnp.dot(dense_hidden, dense_down, preferred_element_type=jnp.float32)
    blend = jax.nn.sigmoid(lax.optimization_barrier(jnp.sum(normed2.astype(jnp.float32) * blend_weight, axis=-1)))
    layer_out = (resid.astype(jnp.float32) + routed + blend[:, None] * dense).astype(jnp.bfloat16)
    return (layer_out, matrix, norm_vec, new_max)
```

```python
import functools

import jax
import jax.numpy as jnp
from jax import lax
from jax.experimental import pallas as pl
from jax.experimental.pallas import tpu as pltpu
from jax.sharding import PartitionSpec as P

epsilon = 1e-06
F32 = jnp.float32
BF16 = jnp.bfloat16
MESH = pl.DeviceIdType.MESH
LANES = 128


def rms_rows(floats, gains):
    scaled = floats * lax.rsqrt(jnp.mean(floats * floats, axis=-1, keepdims=True) + epsilon)
    return (scaled * gains).astype(BF16)


def silu(x):
    return x / (1.0 + jnp.exp(-x))


def sigmoid(x):
    return 1.0 / (1.0 + jnp.exp(-x))


def eye_mask(n):
    return lax.broadcasted_iota(jnp.int32, (n, n), 0) == lax.broadcasted_iota(jnp.int32, (n, n), 1)


def to_column(row):
    return jnp.sum(jnp.where(eye_mask(row.shape[1]), row, 0.0), axis=1, keepdims=True)


def to_row(column):
    return jnp.sum(jnp.where(eye_mask(column.shape[0]), column, 0.0), axis=0, keepdims=True)


def dot_nt(a, b):
    return lax.dot_general(a, b, (((1,), (1,)), ((), ())), preferred_element_type=F32)


def flush_kernel(*refs):
    count = (len(refs) - 1) // 2
    copies = [
        pltpu.make_async_copy(refs[i], refs[count + i], refs[-1].at[i]) for i in range(count)
    ]
    for copy in copies:
        copy.start()
    for copy in copies:
        copy.wait()


def whole(ref, sem):
    return pltpu.make_async_copy(ref, ref, sem)


def flipped(me, k):
    peer, bit = me, 1
    while bit <= k:
        if k & bit:
            peer = peer + bit * (1 - 2 * ((me // bit) % 2))
        bit *= 2
    return peer


def feed_kernel(
    n_ep, n_tp, chunk, small, *refs,
):
    (
        tokens_hbm, wi_hbm, wf_hbm, bias_hbm, head_gain_hbm, mixer_gain_hbm, old_norm_hbm, old_max_hbm,
        feed_gain_hbm, blend_hbm, routes_hbm, scores_hbm,
    ) = refs[:small]
    (
        wq, wk, wv, wo, matrix_hbm, merge_hbm, gate_hbm, up_hbm, down_hbm, left_hbm, right_hbm, ddown_hbm,
        out, new_matrix, new_norm, new_max,
        wquery, wbuf, mbuf, spread, numer, aux, merge, gate_up, down, sides, ddown,
        head_send, head_recv, resid_buf, norm_buf, route_buf, route_all, route_far, every,
        hidden, part_send, part_recv, dense, ret_send, ret_recv,
        msem, wsem, head_sem, route_sem, ag_sem, ag_rsem, fwd_sem, part_sem, ret_sem,
    ) = refs[small : -small - 1]
    held, small_sems = refs[-small - 1 : -1], refs[-1]
    (
        tokens, wi, wf, bias, head_gain, mixer_gain, old_norm, old_max, feed_gain, blend_weight,
        routes, scores,
    ) = held

    small_copies = [
        pltpu.make_async_copy(refs[i], held[i], small_sems.at[i]) for i in range(small)
    ]
    wcopies = [
        pltpu.make_async_copy(ref, wbuf.at[i], wsem.at[0]) for i, ref in enumerate((wk, wv, wo))
    ]
    query_copy = pltpu.make_async_copy(wq, wquery, wsem.at[6])
    for copy in small_copies:
        copy.start()
    query_copy.start()

    me = lax.axis_index("ep")
    core = lax.axis_index("tp")
    partner = {"tp": 1 - core}
    rows, width = tokens.shape
    half = rows // n_tp
    hub = n_tp - 1
    side = n_ep // 2
    peers = {k: flipped(me, k) for k in range(1, n_ep)}
    far_ks, near_ks = list(range(n_ep - 1, side - 1, -1)), list(range(side - 1, 0, -1))
    near_first = (me // side) * side
    far_first = side - near_first

    barrier = pltpu.get_barrier_semaphore()
    pl.semaphore_signal(barrier, inc=1, device_id=partner, device_id_type=MESH)
    for k in far_ks + near_ks:
        pl.semaphore_signal(
            barrier, inc=1, device_id={"ep": peers[k], "tp": hub if k >= side else 0}, device_id_type=MESH
        )
    for copy in wcopies:
        copy.start()

    chunks = rows // chunk
    mcopies = [
        pltpu.make_async_copy(
            matrix_hbm.at[pl.ds(c * chunk, chunk)], mbuf.at[pl.ds(c * chunk, chunk)], msem.at[c]
        )
        for c in range(chunks)
    ]
    merge_copy = pltpu.make_async_copy(merge_hbm, merge, wsem.at[1])
    side_copies = [
        pltpu.make_async_copy(ref, sides.at[i], wsem.at[2]) for i, ref in enumerate((left_hbm, right_hbm))
    ]
    down_copy = pltpu.make_async_copy(down_hbm.at[0], down, wsem.at[3])
    ddown_copy = pltpu.make_async_copy(ddown_hbm, ddown, wsem.at[4])
    tiles = gate_up.shape[0]
    gu_copies = []
    for j in range(tiles):
        for column, ref in enumerate((gate_hbm, up_hbm)):
            gu_copies.append(
                pltpu.make_async_copy(
                    ref.at[0, :, pl.ds(j * LANES, LANES)],
                    gate_up.at[j, :, pl.ds(column * LANES, LANES)],
                    wsem.at[5],
                )
            )
    for copy in small_copies:
        copy.wait()
    for copy in mcopies + [merge_copy]:
        copy.start()

    heads, size = head_gain.shape
    inner = heads * size
    mixed = rms_rows(tokens[...].astype(F32), mixer_gain[...])
    mixed_f = mixed.astype(F32)
    keeps, writes, maxes = [], [], []
    for h in range(heads):
        in_gate = jnp.sum(mixed_f * wi[h : h + 1, :].astype(F32), axis=-1, keepdims=True)
        pre = jnp.sum(mixed_f * wf[h : h + 1, :].astype(F32), axis=-1, keepdims=True) + bias[:, h : h + 1]
        log_forget = jnp.minimum(pre, 0.0) - jnp.log1p(jnp.exp(-jnp.abs(pre)))
        old = to_column(old_max[h : h + 1, :])
        top = jnp.maximum(log_forget + old, in_gate)
        keeps.append(jnp.exp(log_forget + old - top))
        writes.append(jnp.exp(in_gate - top))
        maxes.append(top)

    query_copy.wait()
    query = jnp.dot(mixed, wquery[...], preferred_element_type=F32)
    high = query.astype(BF16)
    rest = query - high.astype(F32)
    middle = rest.astype(BF16)
    low = (rest - middle.astype(F32)).astype(BF16)
    terms = jnp.concatenate([high, middle, low], axis=0)
    lines = lax.broadcasted_iota(jnp.int32, (3 * rows, rows * size), 0)
    columns = lax.broadcasted_iota(jnp.int32, (3 * rows, rows * size), 1)
    pick = jnp.where(lax.rem(lines, rows) == columns // size, 1.0, 0.0).astype(BF16)
    spread[...] = lax.dot_general(
        terms, pick, (((0,), (0,)), ((), ())), preferred_element_type=F32
    )

    whole(wbuf, wsem.at[0]).wait()

    def project(i):
        return jnp.dot(mixed, wbuf[i], preferred_element_type=F32)

    keys = project(0) * size ** (-0.5)
    values = project(1)
    outgate = project(2)
    aux[:, :inner] = values
    denoms, crosses = [], []
    for h in range(heads):
        span = slice(h * size, (h + 1) * size)
        written = writes[h] * keys[:, span]
        aux[:, inner + h * size : inner + (h + 1) * size] = written
        fresh = keeps[h] * old_norm[:, h, :] + written
        new_norm[:, h, :] = fresh
        denoms.append(jnp.sum(query[:, span] * fresh, axis=-1, keepdims=True))
        crosses.append(jnp.sum(query[:, span] * written, axis=-1, keepdims=True))
    for c in range(chunks):
        mcopies[c].wait()
        for b in range(c * chunk, (c + 1) * chunk):
            for h in range(heads):
                numer[b : b + 1, h * size : (h + 1) * size] = jnp.sum(
                    spread[h * size : (h + 1) * size, b * size : (b + 1) * size] * mbuf[b, h],
                    axis=0,
                    keepdims=True,
                )
    energy = jnp.zeros((rows, 1), F32)
    gated = []
    for h in range(heads):
        span = slice(h * size, (h + 1) * size)
        readout = (keeps[h] * numer[:, span] + crosses[h] * values[:, span]) / jnp.maximum(
            jnp.abs(denoms[h]), jnp.exp(-maxes[h])
        )
        energy = energy + jnp.sum(readout * readout, axis=-1, keepdims=True)
        gated.append(
            (readout * head_gain[h : h + 1, :] * sigmoid(outgate[:, span])).astype(BF16)
        )
    merge_copy.wait()
    head_part = jnp.dot(
        jnp.concatenate(gated, axis=1), merge[...], preferred_element_type=F32
    )
    head_send[:, :width] = head_part
    head_send[:, width:] = jnp.broadcast_to(energy, (rows, LANES))

    @pl.when(core == hub)
    def _():
        pl.semaphore_wait(barrier, 2 * len(far_ks) + 1)

    @pl.when(core != hub)
    def _():
        pl.semaphore_wait(barrier, 2 * len(near_ks) + 1)

    head_copy = pltpu.make_async_remote_copy(
        head_send, head_recv, head_sem.at[0], head_sem.at[1], device_id=partner, device_id_type=MESH
    )
    head_copy.start()
    for copy in gu_copies + [down_copy]:
        copy.start()

    @pl.when(core == hub)
    def _():
        for copy in side_copies + [ddown_copy]:
            copy.start()

    def send(source, slot, send_sem, recv_sem, device):
        pltpu.make_async_remote_copy(
            source, slot, send_sem, recv_sem, device_id=device, device_id_type=MESH
        ).start()

    def all_others(slots, sem):
        return whole(slots.at[pl.ds(0, n_ep - 1)], sem)

    picks = routes.shape[0]
    score = scores[...].astype(F32)
    raised = jnp.exp(score - jnp.max(score, axis=0, keepdims=True))
    route_weight = raised / jnp.sum(raised, axis=0, keepdims=True)
    chosen = routes[...]
    route_buf[...] = jnp.zeros_like(route_buf)
    for e in range(n_ep):
        named = jnp.zeros((1, rows), F32)
        for p in range(picks):
            named = named + jnp.where(chosen[p : p + 1, :] == e, route_weight[p : p + 1, :], 0.0)
        route_buf[e, :, :rows] = named
    for h in range(heads):
        new_max[h : h + 1, :] = to_row(maxes[h])

    head_copy.wait()
    head_total = head_part + head_recv[:, :width]
    energy_total = energy + head_recv[:, width : width + 1]
    scale = lax.rsqrt(energy_total / (inner * n_tp) + epsilon)
    resid = (tokens[...].astype(F32) + scale * head_total).astype(BF16).astype(F32)
    norm_buf[...] = rms_rows(resid, feed_gain[...])

    def spread_rows(ks):
        for k in ks:
            send(norm_buf, every.at[me], ag_sem, ag_rsem.at[me], {"ep": peers[k], "tp": hub})
        for k in ks:
            send(
                route_buf.at[peers[k]], route_all.at[me], route_sem.at[0], route_sem.at[1],
                {"ep": peers[k], "tp": hub},
            )

    @pl.when(core == hub)
    def _():
        spread_rows(far_ks)

    @pl.when(core != hub)
    def _():
        spread_rows(near_ks)

    every[me] = norm_buf[...]
    route_all[me] = route_buf[me]

    for i in range(n_tp):
        resid_buf[i] = resid[i * half : (i + 1) * half]

    for h in range(heads):
        key_cols = aux[:, inner + h * size : inner + (h + 1) * size].T
        for b in range(rows):
            new_matrix[b, h] = (
                keeps[h][b : b + 1, :] * mbuf[b, h]
                + key_cols[:, b : b + 1] * aux[b : b + 1, h * size : (h + 1) * size]
            )

    @pl.when(core == hub)
    def _():
        for i in range(n_ep - 1):
            origin = i + (i - me + n_ep) // n_ep
            whole(every.at[origin], ag_rsem.at[origin]).wait()
            send(every.at[origin], every.at[origin], fwd_sem.at[0], fwd_sem.at[1], partner)

    @pl.when(core != hub)
    def _():
        all_others(every, fwd_sem.at[1]).wait()

    count = n_ep * rows
    whole(gate_up, wsem.at[5]).wait()
    all_rows = every[...].reshape(count, width)
    for j in range(tiles):
        both = jnp.dot(all_rows, gate_up[j], preferred_element_type=F32)
        hidden[:, j * LANES : (j + 1) * LANES] = (
            silu(both[:, :LANES]) * both[:, LANES:]
        ).astype(BF16)
    down_copy.wait()
    block = count // 2
    near_span = pl.ds(pl.multiple_of(near_first * rows, block), block)
    far_span = pl.ds(pl.multiple_of(far_first * rows, block), block)

    def part_of(span):
        return jnp.dot(hidden[span, :], down[...], preferred_element_type=F32).astype(BF16)

    def weights_of(table, first):
        weights = jnp.broadcast_to(table[pl.ds(first, side)], (side, rows, LANES)).reshape(block, LANES)
        token = lax.rem(lax.broadcasted_iota(jnp.int32, (block, LANES), 0), rows)
        lane = lax.broadcasted_iota(jnp.int32, (block, LANES), 1)
        return jnp.sum(jnp.where(lane == token, weights, 0.0), axis=-1, keepdims=True)

    def give_back(combined, ks, first):
        ret_send[...] = combined.reshape(side, n_tp, half, width).astype(BF16)
        for k in ks:
            for i in range(n_tp):
                send(
                    ret_send.at[peers[k] - first, i], ret_recv.at[me], ret_sem.at[0], ret_sem.at[1],
                    {"ep": peers[k], "tp": i},
                )

    @pl.when(core != hub)
    def _():
        part_send[...] = part_of(far_span)
        send(part_send, part_recv, part_sem.at[0], part_sem.at[1], partner)
        part = part_of(near_span).astype(F32)
        whole(route_far, route_sem.at[3]).wait()
        own_weight = weights_of(route_far, near_first)
        whole(part_recv, part_sem.at[1]).wait()
        give_back(own_weight * part + part_recv[...].astype(F32), near_ks, near_first)
        send(ret_send.at[me - near_first, hub], ret_recv.at[me], ret_sem.at[0], ret_sem.at[1], partner)
        ret_recv[me] = ret_send[me - near_first, 0]
        if near_ks:
            whole(route_all.at[pl.ds(0, side - 1)], route_sem.at[0]).wait()
            whole(every.at[pl.ds(0, side - 1)], ag_sem).wait()
        whole(part_send, part_sem.at[0]).wait()
        all_others(ret_recv, ret_sem.at[1]).wait()

    @pl.when(core == hub)
    def _():
        all_others(route_all, route_sem.at[1]).wait()
        send(route_all, route_far, route_sem.at[2], route_sem.at[3], partner)
        near_part = part_of(near_span).astype(F32)
        whole(sides, wsem.at[2]).wait()
        ddown_copy.wait()
        inputs = every[...].reshape(count, width)
        blend = sigmoid(jnp.sum(inputs.astype(F32) * blend_weight[...], axis=-1, keepdims=True))
        dense_hidden = (silu(dot_nt(inputs, sides[0])) * dot_nt(inputs, sides[1])).astype(BF16)
        dense[...] = blend * jnp.dot(dense_hidden, ddown[...], preferred_element_type=F32)
        part_send[...] = (weights_of(route_all, near_first) * near_part + dense[near_span, :]).astype(BF16)
        send(part_send, part_recv, part_sem.at[0], part_sem.at[1], partner)
        part = part_of(far_span).astype(F32)
        own_weight = weights_of(route_all, far_first)
        whole(part_recv, part_sem.at[1]).wait()
        expert_out = (part + part_recv[...].astype(F32)).astype(BF16).astype(F32)
        give_back(own_weight * expert_out + dense[far_span, :], far_ks, far_first)
        whole(route_all.at[pl.ds(0, side)], route_sem.at[0]).wait()
        whole(route_all, route_sem.at[2]).wait()
        whole(every.at[pl.ds(0, side)], ag_sem).wait()
        all_others(every, fwd_sem.at[0]).wait()
        whole(part_send, part_sem.at[0]).wait()
        whole(ret_recv, ret_sem.at[1]).wait()

    total = resid_buf[core]
    for e in range(n_ep):
        total = total + ret_recv[e].astype(F32)
    out[...] = total.astype(BF16)

    @pl.when(core == hub)
    def _():
        whole(ret_recv, ret_sem.at[0]).wait()

    @pl.when(core != hub)
    def _():
        all_others(ret_recv, ret_sem.at[0]).wait()


VMEM = pl.BlockSpec(memory_space=pltpu.VMEM)
ANY = pl.BlockSpec(memory_space=pl.ANY)


def local(
    n_ep, n_tp, tokens, query_weight, key_weight, value_weight, outgate_weight, ingate_weight,
    forget_weight, forget_bias, head_gain, merge_weight, mixer_gain, feed_gain, memory_matrix,
    memory_norm, memory_max, routes, route_scores, expert_gate, expert_up, expert_down,
    dense_left, dense_right, dense_down, blend_weight,
):
    rows, width = tokens.shape
    heads, size = head_gain.shape
    half = rows // n_tp
    chunk = max(1, rows // 2)
    chunks = rows // chunk
    dma = pltpu.SemaphoreType.DMA
    inner = expert_gate.shape[2]
    tiles = inner // LANES
    dense_inner = dense_left.shape[1]
    count = n_ep * rows
    lanes = heads * size
    small = (
        tokens, ingate_weight.T, forget_weight.T, forget_bias.reshape(1, heads), head_gain,
        mixer_gain.reshape(1, width), memory_norm, memory_max.T, feed_gain.reshape(1, width),
        blend_weight.reshape(1, width), routes.T, route_scores.T,
    )
    operands = (
        *small, query_weight, key_weight, value_weight, outgate_weight, memory_matrix, merge_weight, expert_gate, expert_up,
        expert_down, dense_left.T, dense_right.T, dense_down,
    )
    layer_half, matrix, norm_vec, new_max = pl.pallas_call(
        functools.partial(feed_kernel, n_ep, n_tp, chunk, len(small)),
        out_shape=(
            pltpu.VMEM((half, width), BF16),
            pltpu.VMEM(memory_matrix.shape, F32),
            pltpu.VMEM(memory_norm.shape, F32),
            pltpu.VMEM((heads, rows), F32),
        ),
        in_specs=[ANY] * (len(small) + 12),
        out_specs=(VMEM,) * 4,
        scratch_shapes=[
            pltpu.VMEM((width, lanes), BF16),
            pltpu.VMEM((3, width, lanes), BF16),
            pltpu.VMEM(memory_matrix.shape, F32),
            pltpu.VMEM((lanes, rows * size), F32),
            pltpu.VMEM((rows, lanes), F32),
            pltpu.VMEM((rows, 2 * lanes), F32),
            pltpu.VMEM(merge_weight.shape, BF16),
            pltpu.VMEM((tiles, width, 2 * LANES), BF16),
            pltpu.VMEM((inner, width), BF16),
            pltpu.VMEM((2, dense_inner, width), BF16),
            pltpu.VMEM((dense_inner, width), BF16),
            pltpu.VMEM((rows, width + LANES), F32),
            pltpu.VMEM((rows, width + LANES), F32),
            pltpu.VMEM((n_tp, half, width), F32),
            pltpu.VMEM((rows, width), BF16),
            pltpu.VMEM((n_ep, 1, LANES), F32),
            pltpu.VMEM((n_ep, 1, LANES), F32),
            pltpu.VMEM((n_ep, 1, LANES), F32),
            pltpu.VMEM((n_ep, rows, width), BF16),
            pltpu.VMEM((count, inner), BF16),
            pltpu.VMEM((count // 2, width), BF16),
            pltpu.VMEM((count // 2, width), BF16),
            pltpu.VMEM((count, width), F32),
            pltpu.VMEM((n_ep // 2, n_tp, half, width), BF16),
            pltpu.VMEM((n_ep, half, width), BF16),
            dma((chunks,)),
            dma((7,)),
            dma((2,)),
            dma((4,)),
            dma,
            dma((n_ep,)),
            dma((2,)),
            dma((2,)),
            dma((2,)),
            *(pltpu.VMEM(a.shape, a.dtype) for a in small),
            dma((len(small),)),
        ],
        compiler_params=pltpu.CompilerParams(
            collective_id=0, has_side_effects=True, vmem_limit_bytes=48 << 20
        ),
        name="feed_forward",
    )(*(pltpu.with_memory_space_constraint(a, pltpu.HBM) for a in operands))
    held = (layer_half, matrix, norm_vec, new_max)
    layer_out, matrix, norm_vec, new_max = pl.pallas_call(
        flush_kernel,
        out_shape=tuple(jax.ShapeDtypeStruct(a.shape, a.dtype) for a in held),
        in_specs=[VMEM] * 4,
        out_specs=(ANY,) * 4,
        scratch_shapes=[dma((4,))],
        compiler_params=pltpu.CompilerParams(vmem_limit_bytes=8 << 20),
        name="write_out",
    )(*held)
    return (layer_out, matrix, norm_vec, new_max.T)


def solution(mesh):
    row = ("grp", "ep")
    in_specs = (
        P(row, None),
        P(None, "tp"),
        P(None, "tp"),
        P(None, "tp"),
        P(None, "tp"),
        P(None, "tp"),
        P(None, "tp"),
        P("tp"),
        P("tp", None),
        P("tp", None),
        P(),
        P(),
        P(row, "tp", None, None),
        P(row, "tp", None),
        P(row, "tp"),
        P(row, None),
        P(row, None),
        P("ep", None, "tp"),
        P("ep", None, "tp"),
        P("ep", "tp", None),
        P(None, "ep"),
        P(None, "ep"),
        P("ep", None),
        P(),
    )
    out_specs = (
        P(("grp", "ep", "tp"), None),
        P(row, "tp", None, None),
        P(row, "tp", None),
        P(row, "tp"),
    )
    body = functools.partial(local, mesh.shape["ep"], mesh.shape["tp"])
    return jax.shard_map(body, mesh=mesh, in_specs=in_specs, out_specs=out_specs, check_vma=False)
```

```python
import functools

import jax
import jax.numpy as jnp
from jax import lax
from jax.experimental import pallas as pl
from jax.experimental.pallas import tpu as pltpu
from jax.sharding import PartitionSpec as P

epsilon = 1e-06
F32 = jnp.float32
BF16 = jnp.bfloat16
MESH = pl.DeviceIdType.MESH
LANES = 128


def rms_rows(floats, gains):
    scaled = floats * lax.rsqrt(jnp.mean(floats * floats, axis=-1, keepdims=True) + epsilon)
    return (scaled * gains).astype(BF16)


def silu(x):
    return x / (1.0 + jnp.exp(-x))


def sigmoid(x):
    return 1.0 / (1.0 + jnp.exp(-x))


def eye_mask(n):
    return lax.broadcasted_iota(jnp.int32, (n, n), 0) == lax.broadcasted_iota(jnp.int32, (n, n), 1)


def to_column(row):
    return jnp.sum(jnp.where(eye_mask(row.shape[1]), row, 0.0), axis=1, keepdims=True)


def to_row(column):
    return jnp.sum(jnp.where(eye_mask(column.shape[0]), column, 0.0), axis=0, keepdims=True)


def dot_nt(a, b):
    return lax.dot_general(a, b, (((1,), (1,)), ((), ())), preferred_element_type=F32)


def flush_kernel(*refs):
    count = (len(refs) - 1) // 2
    copies = [
        pltpu.make_async_copy(refs[i], refs[count + i], refs[-1].at[i]) for i in range(count)
    ]
    for copy in copies:
        copy.start()
    for copy in copies:
        copy.wait()


def whole(ref, sem):
    return pltpu.make_async_copy(ref, ref, sem)


def flipped(me, k):
    peer, bit = me, 1
    while bit <= k:
        if k & bit:
            peer = peer + bit * (1 - 2 * ((me // bit) % 2))
        bit *= 2
    return peer


def feed_kernel(
    n_ep, n_tp, chunk, small, *refs,
):
    (
        tokens_hbm, wi_hbm, wf_hbm, bias_hbm, head_gain_hbm, mixer_gain_hbm, old_norm_hbm, old_max_hbm,
        feed_gain_hbm, blend_hbm, routes_hbm, scores_hbm,
    ) = refs[:small]
    (
        wq, wk, wv, wo, matrix_hbm, merge_hbm, gate_hbm, up_hbm, down_hbm, left_hbm, right_hbm, ddown_hbm,
        out, new_matrix, new_norm, new_max,
        wquery, wbuf, mbuf, spread, numer, aux, merge, gate_up, down, sides, ddown,
        head_send, head_recv, resid_buf, norm_buf, route_buf, route_all, route_far, every,
        hidden, part_send, part_recv, dense, ret_send, ret_recv,
        msem, wsem, head_sem, route_sem, ag_sem, ag_rsem, fwd_sem, part_sem, ret_sem,
    ) = refs[small : -small - 1]
    held, small_sems = refs[-small - 1 : -1], refs[-1]
    (
        tokens, wi, wf, bias, head_gain, mixer_gain, old_norm, old_max, feed_gain, blend_weight,
        routes, scores,
    ) = held

    small_copies = [
        pltpu.make_async_copy(refs[i], held[i], small_sems.at[i]) for i in range(small)
    ]
    wcopies = [
        pltpu.make_async_copy(ref, wbuf.at[i], wsem.at[0]) for i, ref in enumerate((wk, wv, wo))
    ]
    query_copy = pltpu.make_async_copy(wq, wquery, wsem.at[6])
    for copy in small_copies:
        copy.start()
    query_copy.start()

    me = lax.axis_index("ep")
    core = lax.axis_index("tp")
    partner = {"tp": 1 - core}
    rows, width = tokens.shape
    half = rows // n_tp
    hub = n_tp - 1
    side = n_ep // 2
    peers = {k: flipped(me, k) for k in range(1, n_ep)}
    far_ks, near_ks = list(range(n_ep - 1, side - 1, -1)), list(range(side - 1, 0, -1))
    near_first = (me // side) * side
    far_first = side - near_first

    barrier = pltpu.get_barrier_semaphore()
    pl.semaphore_signal(barrier, inc=1, device_id=partner, device_id_type=MESH)
    for k in far_ks + near_ks:
        pl.semaphore_signal(
            barrier, inc=1, device_id={"ep": peers[k], "tp": hub if k >= side else 0}, device_id_type=MESH
        )
    for copy in wcopies:
        copy.start()

    chunks = rows // chunk
    mcopies = [
        pltpu.make_async_copy(
            matrix_hbm.at[pl.ds(c * chunk, chunk)], mbuf.at[pl.ds(c * chunk, chunk)], msem.at[c]
        )
        for c in range(chunks)
    ]
    merge_copy = pltpu.make_async_copy(merge_hbm, merge, wsem.at[1])
    side_copies = [
        pltpu.make_async_copy(ref, sides.at[i], wsem.at[2]) for i, ref in enumerate((left_hbm, right_hbm))
    ]
    down_copy = pltpu.make_async_copy(down_hbm.at[0], down, wsem.at[3])
    ddown_copy = pltpu.make_async_copy(ddown_hbm, ddown, wsem.at[4])
    tiles = gate_up.shape[0]
    gu_copies = []
    for j in range(tiles):
        for column, ref in enumerate((gate_hbm, up_hbm)):
            gu_copies.append(
                pltpu.make_async_copy(
                    ref.at[0, :, pl.ds(j * LANES, LANES)],
                    gate_up.at[j, :, pl.ds(column * LANES, LANES)],
                    wsem.at[5],
                )
            )
    for copy in small_copies:
        copy.wait()
    for copy in mcopies + [merge_copy]:
        copy.start()

    heads, size = head_gain.shape
    inner = heads * size
    mixed = rms_rows(tokens[...].astype(F32), mixer_gain[...])
    mixed_f = mixed.astype(F32)
    keeps, writes, maxes = [], [], []
    for h in range(heads):
        in_gate = jnp.sum(mixed_f * wi[h : h + 1, :].astype(F32), axis=-1, keepdims=True)
        pre = jnp.sum(mixed_f * wf[h : h + 1, :].astype(F32), axis=-1, keepdims=True) + bias[:, h : h + 1]
        log_forget = jnp.minimum(pre, 0.0) - jnp.log1p(jnp.exp(-jnp.abs(pre)))
        old = to_column(old_max[h : h + 1, :])
        top = jnp.maximum(log_forget + old, in_gate)
        keeps.append(jnp.exp(log_forget + old - top))
        writes.append(jnp.exp(in_gate - top))
        maxes.append(top)

    query_copy.wait()
    query = jnp.dot(mixed, wquery[...], preferred_element_type=F32)
    high = query.astype(BF16)
    rest = query - high.astype(F32)
    middle = rest.astype(BF16)
    low = (rest - middle.astype(F32)).astype(BF16)
    terms = jnp.concatenate([high, middle, low], axis=0)
    lines = lax.broadcasted_iota(jnp.int32, (3 * rows, rows * size), 0)
    columns = lax.broadcasted_iota(jnp.int32, (3 * rows, rows * size), 1)
    pick = jnp.where(lax.rem(lines, rows) == columns // size, 1.0, 0.0).astype(BF16)
    spread[...] = lax.dot_general(
        terms, pick, (((0,), (0,)), ((), ())), preferred_element_type=F32
    )

    whole(wbuf, wsem.at[0]).wait()

    def project(i):
        return jnp.dot(mixed, wbuf[i], preferred_element_type=F32)

    keys = project(0) * size ** (-0.5)
    values = project(1)
    outgate = project(2)
    aux[:, :inner] = values
    denoms, crosses = [], []
    for h in range(heads):
        span = slice(h * size, (h + 1) * size)
        written = writes[h] * keys[:, span]
        aux[:, inner + h * size : inner + (h + 1) * size] = written
        fresh = keeps[h] * old_norm[:, h, :] + written
        new_norm[:, h, :] = fresh
        denoms.append(jnp.sum(query[:, span] * fresh, axis=-1, keepdims=True))
        crosses.append(jnp.sum(query[:, span] * written, axis=-1, keepdims=True))
    for c in range(chunks):
        mcopies[c].wait()
        for b in range(c * chunk, (c + 1) * chunk):
            for h in range(heads):
                numer[b : b + 1, h * size : (h + 1) * size] = jnp.sum(
                    spread[h * size : (h + 1) * size, b * size : (b + 1) * size] * mbuf[b, h],
                    axis=0,
                    keepdims=True,
                )
    energy = jnp.zeros((rows, 1), F32)
    gated = []
    for h in range(heads):
        span = slice(h * size, (h + 1) * size)
        readout = (keeps[h] * numer[:, span] + crosses[h] * values[:, span]) / jnp.maximum(
            jnp.abs(denoms[h]), jnp.exp(-maxes[h])
        )
        energy = energy + jnp.sum(readout * readout, axis=-1, keepdims=True)
        gated.append(
            (readout * head_gain[h : h + 1, :] * sigmoid(outgate[:, span])).astype(BF16)
        )
    merge_copy.wait()
    head_part = jnp.dot(
        jnp.concatenate(gated, axis=1), merge[...], preferred_element_type=F32
    )
    head_send[:, :width] = head_part
    head_send[:, width:] = jnp.broadcast_to(energy, (rows, LANES))

    @pl.when(core == hub)
    def _():
        pl.semaphore_wait(barrier, 2 * len(far_ks) + 1)

    @pl.when(core != hub)
    def _():
        pl.semaphore_wait(barrier, 2 * len(near_ks) + 1)

    head_copy = pltpu.make_async_remote_copy(
        head_send, head_recv, head_sem.at[0], head_sem.at[1], device_id=partner, device_id_type=MESH
    )
    head_copy.start()
    for copy in gu_copies + [down_copy]:
        copy.start()

    @pl.when(core == hub)
    def _():
        for copy in side_copies + [ddown_copy]:
            copy.start()

    def send(source, slot, send_sem, recv_sem, device):
        pltpu.make_async_remote_copy(
            source, slot, send_sem, recv_sem, device_id=device, device_id_type=MESH
        ).start()

    def all_others(slots, sem):
        return whole(slots.at[pl.ds(0, n_ep - 1)], sem)

    picks = routes.shape[0]
    score = scores[...].astype(F32)
    raised = jnp.exp(score - jnp.max(score, axis=0, keepdims=True))
    route_weight = raised / jnp.sum(raised, axis=0, keepdims=True)
    chosen = routes[...]
    route_buf[...] = jnp.zeros_like(route_buf)
    for e in range(n_ep):
        named = jnp.zeros((1, rows), F32)
        for p in range(picks):
            named = named + jnp.where(chosen[p : p + 1, :] == e, route_weight[p : p + 1, :], 0.0)
        route_buf[e, :, :rows] = named
    route_all[me] = route_buf[me]

    def spread_routes(ks):
        for k in ks:
            send(
                route_buf.at[peers[k]], route_all.at[me], route_sem.at[0], route_sem.at[1],
                {"ep": peers[k], "tp": hub},
            )

    @pl.when(core == hub)
    def _():
        spread_routes(far_ks)

    @pl.when(core != hub)
    def _():
        spread_routes(near_ks)

    for h in range(heads):
        new_max[h : h + 1, :] = to_row(maxes[h])

    head_copy.wait()
    head_total = head_part + head_recv[:, :width]
    energy_total = energy + head_recv[:, width : width + 1]
    scale = lax.rsqrt(energy_total / (inner * n_tp) + epsilon)
    resid = (tokens[...].astype(F32) + scale * head_total).astype(BF16).astype(F32)
    norm_buf[...] = rms_rows(resid, feed_gain[...])

    def spread_rows(ks):
        for k in ks:
            send(norm_buf, every.at[me], ag_sem, ag_rsem.at[me], {"ep": peers[k], "tp": hub})

    @pl.when(core == hub)
    def _():
        spread_rows(far_ks)

    @pl.when(core != hub)
    def _():
        spread_rows(near_ks)

    every[me] = norm_buf[...]

    for i in range(n_tp):
        resid_buf[i] = resid[i * half : (i + 1) * half]

    for h in range(heads):
        key_cols = aux[:, inner + h * size : inner + (h + 1) * size].T
        for b in range(rows):
            new_matrix[b, h] = (
                keeps[h][b : b + 1, :] * mbuf[b, h]
                + key_cols[:, b : b + 1] * aux[b : b + 1, h * size : (h + 1) * size]
            )

    @pl.when(core == hub)
    def _():
        for i in range(n_ep - 1):
            origin = i + (i - me + n_ep) // n_ep
            whole(every.at[origin], ag_rsem.at[origin]).wait()
            send(every.at[origin], every.at[origin], fwd_sem.at[0], fwd_sem.at[1], partner)

    @pl.when(core != hub)
    def _():
        down_copy.wait()
        whole(gate_up, wsem.at[5]).wait()
        all_others(every, fwd_sem.at[1]).wait()

    count = n_ep * rows
    block = count // 2
    near_span = pl.ds(pl.multiple_of(near_first * rows, block), block)
    far_span = pl.ds(pl.multiple_of(far_first * rows, block), block)

    def fill_hidden():
        all_rows = every[...].reshape(count, width)
        for j in range(tiles):
            both = jnp.dot(all_rows, gate_up[j], preferred_element_type=F32)
            hidden[:, j * LANES : (j + 1) * LANES] = (
                silu(both[:, :LANES]) * both[:, LANES:]
            ).astype(BF16)

    def part_of(span):
        return jnp.dot(hidden[span, :], down[...], preferred_element_type=F32).astype(BF16)

    def weights_of(table, first):
        weights = jnp.broadcast_to(table[pl.ds(first, side)], (side, rows, LANES)).reshape(block, LANES)
        token = lax.rem(lax.broadcasted_iota(jnp.int32, (block, LANES), 0), rows)
        lane = lax.broadcasted_iota(jnp.int32, (block, LANES), 1)
        return jnp.sum(jnp.where(lane == token, weights, 0.0), axis=-1, keepdims=True)

    piece = width // 2
    pieces = [slice(i * piece, (i + 1) * piece) for i in range(2)]

    def give_back(i, combined, ks, first):
        ret_send[i] = combined.reshape(side, n_tp, half, piece).astype(BF16)
        for k in ks:
            for c in range(n_tp):
                send(
                    ret_send.at[i, peers[k] - first, c], ret_recv.at[me, i], ret_sem.at[0], ret_sem.at[1],
                    {"ep": peers[k], "tp": c},
                )

    @pl.when(core != hub)
    def _():
        fill_hidden()
        for i in range(2):
            part_send[i] = jnp.dot(
                hidden[far_span, :], down[:, pieces[i]], preferred_element_type=F32
            ).astype(BF16)
            send(part_send.at[i], part_recv.at[i], part_sem.at[0], part_sem.at[1 + i], partner)
        part = part_of(near_span).astype(F32)
        whole(route_far, route_sem.at[3]).wait()
        own_weight = weights_of(route_far, near_first)
        for i in range(2):
            whole(part_recv.at[i], part_sem.at[1 + i]).wait()
            give_back(i, own_weight * part[:, pieces[i]] + part_recv[i].astype(F32), near_ks, near_first)
            send(
                ret_send.at[i, me - near_first, hub], ret_recv.at[me, i], ret_sem.at[0], ret_sem.at[1], partner
            )
            ret_recv[me, i] = ret_send[i, me - near_first, 0]
        if near_ks:
            whole(route_all.at[pl.ds(0, side - 1)], route_sem.at[0]).wait()
            whole(every.at[pl.ds(0, side - 1)], ag_sem).wait()
        whole(part_send, part_sem.at[0]).wait()
        all_others(ret_recv, ret_sem.at[1]).wait()

    @pl.when(core == hub)
    def _():
        down_copy.wait()
        whole(gate_up, wsem.at[5]).wait()
        whole(sides, wsem.at[2]).wait()
        ddown_copy.wait()
        all_others(route_all, route_sem.at[1]).wait()
        send(route_all, route_far, route_sem.at[2], route_sem.at[3], partner)
        fill_hidden()
        near_part = part_of(near_span).astype(F32)
        part = part_of(far_span).astype(F32)
        inputs = every[...].reshape(count, width)
        blend = sigmoid(jnp.sum(inputs.astype(F32) * blend_weight[...], axis=-1, keepdims=True))
        dense_hidden = (silu(dot_nt(inputs, sides[0])) * dot_nt(inputs, sides[1])).astype(BF16)
        dense[...] = blend * jnp.dot(dense_hidden, ddown[...], preferred_element_type=F32)
        near_sum = (weights_of(route_all, near_first) * near_part + dense[near_span, :]).astype(BF16)
        for i in range(2):
            part_send[i] = near_sum[:, pieces[i]]
            send(part_send.at[i], part_recv.at[i], part_sem.at[0], part_sem.at[1 + i], partner)
        own_weight = weights_of(route_all, far_first)
        for i in range(2):
            whole(part_recv.at[i], part_sem.at[1 + i]).wait()
            expert_out = (part[:, pieces[i]] + part_recv[i].astype(F32)).astype(BF16).astype(F32)
            give_back(i, own_weight * expert_out + dense[far_span, pieces[i]], far_ks, far_first)
        whole(route_all.at[pl.ds(0, side)], route_sem.at[0]).wait()
        whole(route_all, route_sem.at[2]).wait()
        whole(every.at[pl.ds(0, side)], ag_sem).wait()
        all_others(every, fwd_sem.at[0]).wait()
        whole(part_send, part_sem.at[0]).wait()
        whole(ret_recv, ret_sem.at[1]).wait()

    for i in range(2):
        total = resid_buf[core, :, pieces[i]]
        for e in range(n_ep):
            total = total + ret_recv[e, i].astype(F32)
        out[:, pieces[i]] = total.astype(BF16)

    @pl.when(core == hub)
    def _():
        whole(ret_recv, ret_sem.at[0]).wait()

    @pl.when(core != hub)
    def _():
        all_others(ret_recv, ret_sem.at[0]).wait()


VMEM = pl.BlockSpec(memory_space=pltpu.VMEM)
ANY = pl.BlockSpec(memory_space=pl.ANY)


def local(
    n_ep, n_tp, tokens, query_weight, key_weight, value_weight, outgate_weight, ingate_weight,
    forget_weight, forget_bias, head_gain, merge_weight, mixer_gain, feed_gain, memory_matrix,
    memory_norm, memory_max, routes, route_scores, expert_gate, expert_up, expert_down,
    dense_left, dense_right, dense_down, blend_weight,
):
    rows, width = tokens.shape
    heads, size = head_gain.shape
    half = rows // n_tp
    chunk = max(1, rows // 2)
    chunks = rows // chunk
    dma = pltpu.SemaphoreType.DMA
    inner = expert_gate.shape[2]
    tiles = inner // LANES
    dense_inner = dense_left.shape[1]
    count = n_ep * rows
    lanes = heads * size
    small = (
        tokens, ingate_weight.T, forget_weight.T, forget_bias.reshape(1, heads), head_gain,
        mixer_gain.reshape(1, width), memory_norm, memory_max.T, feed_gain.reshape(1, width),
        blend_weight.reshape(1, width), routes.T, route_scores.T,
    )
    operands = (
        *small, query_weight, key_weight, value_weight, outgate_weight, memory_matrix, merge_weight, expert_gate, expert_up,
        expert_down, dense_left.T, dense_right.T, dense_down,
    )
    layer_half, matrix, norm_vec, new_max = pl.pallas_call(
        functools.partial(feed_kernel, n_ep, n_tp, chunk, len(small)),
        out_shape=(
            pltpu.VMEM((half, width), BF16),
            pltpu.VMEM(memory_matrix.shape, F32),
            pltpu.VMEM(memory_norm.shape, F32),
            pltpu.VMEM((heads, rows), F32),
        ),
        in_specs=[ANY] * (len(small) + 12),
        out_specs=(VMEM,) * 4,
        scratch_shapes=[
            pltpu.VMEM((width, lanes), BF16),
            pltpu.VMEM((3, width, lanes), BF16),
            pltpu.VMEM(memory_matrix.shape, F32),
            pltpu.VMEM((lanes, rows * size), F32),
            pltpu.VMEM((rows, lanes), F32),
            pltpu.VMEM((rows, 2 * lanes), F32),
            pltpu.VMEM(merge_weight.shape, BF16),
            pltpu.VMEM((tiles, width, 2 * LANES), BF16),
            pltpu.VMEM((inner, width), BF16),
            pltpu.VMEM((2, dense_inner, width), BF16),
            pltpu.VMEM((dense_inner, width), BF16),
            pltpu.VMEM((rows, width + LANES), F32),
            pltpu.VMEM((rows, width + LANES), F32),
            pltpu.VMEM((n_tp, half, width), F32),
            pltpu.VMEM((rows, width), BF16),
            pltpu.VMEM((n_ep, 1, LANES), F32),
            pltpu.VMEM((n_ep, 1, LANES), F32),
            pltpu.VMEM((n_ep, 1, LANES), F32),
            pltpu.VMEM((n_ep, rows, width), BF16),
            pltpu.VMEM((count, inner), BF16),
            pltpu.VMEM((2, count // 2, width // 2), BF16),
            pltpu.VMEM((2, count // 2, width // 2), BF16),
            pltpu.VMEM((count, width), F32),
            pltpu.VMEM((2, n_ep // 2, n_tp, half, width // 2), BF16),
            pltpu.VMEM((n_ep, 2, half, width // 2), BF16),
            dma((chunks,)),
            dma((7,)),
            dma((2,)),
            dma((4,)),
            dma,
            dma((n_ep,)),
            dma((2,)),
            dma((3,)),
            dma((2,)),
            *(pltpu.VMEM(a.shape, a.dtype) for a in small),
            dma((len(small),)),
        ],
        compiler_params=pltpu.CompilerParams(
            collective_id=0, has_side_effects=True, vmem_limit_bytes=48 << 20
        ),
        name="feed_forward",
    )(*(pltpu.with_memory_space_constraint(a, pltpu.HBM) for a in operands))
    held = (layer_half, matrix, norm_vec, new_max)
    layer_out, matrix, norm_vec, new_max = pl.pallas_call(
        flush_kernel,
        out_shape=tuple(jax.ShapeDtypeStruct(a.shape, a.dtype) for a in held),
        in_specs=[VMEM] * 4,
        out_specs=(ANY,) * 4,
        scratch_shapes=[dma((4,))],
        compiler_params=pltpu.CompilerParams(vmem_limit_bytes=8 << 20),
        name="write_out",
    )(*held)
    return (layer_out, matrix, norm_vec, new_max.T)


def solution(mesh):
    row = ("grp", "ep")
    in_specs = (
        P(row, None),
        P(None, "tp"),
        P(None, "tp"),
        P(None, "tp"),
        P(None, "tp"),
        P(None, "tp"),
        P(None, "tp"),
        P("tp"),
        P("tp", None),
        P("tp", None),
        P(),
        P(),
        P(row, "tp", None, None),
        P(row, "tp", None),
        P(row, "tp"),
        P(row, None),
        P(row, None),
        P("ep", None, "tp"),
        P("ep", None, "tp"),
        P("ep", "tp", None),
        P(None, "ep"),
        P(None, "ep"),
        P("ep", None),
        P(),
    )
    out_specs = (
        P(("grp", "ep", "tp"), None),
        P(row, "tp", None, None),
        P(row, "tp", None),
        P(row, "tp"),
    )
    body = functools.partial(local, mesh.shape["ep"], mesh.shape["tp"])
    return jax.shard_map(body, mesh=mesh, in_specs=in_specs, out_specs=out_specs, check_vma=False)
```

```python
import functools

import jax
import jax.numpy as jnp
from jax import lax
from jax.experimental import pallas as pl
from jax.experimental.pallas import tpu as pltpu
from jax.sharding import PartitionSpec as P

epsilon = 1e-06
F32 = jnp.float32
BF16 = jnp.bfloat16
MESH = pl.DeviceIdType.MESH
LANES = 128


def rms_rows(floats, gains):
    scaled = floats * lax.rsqrt(jnp.mean(floats * floats, axis=-1, keepdims=True) + epsilon)
    return (scaled * gains).astype(BF16)


def silu(x):
    return x / (1.0 + jnp.exp(-x))


def sigmoid(x):
    return 1.0 / (1.0 + jnp.exp(-x))


def eye_mask(n):
    return lax.broadcasted_iota(jnp.int32, (n, n), 0) == lax.broadcasted_iota(jnp.int32, (n, n), 1)


def to_column(row):
    return jnp.sum(jnp.where(eye_mask(row.shape[1]), row, 0.0), axis=1, keepdims=True)


def to_row(column):
    return jnp.sum(jnp.where(eye_mask(column.shape[0]), column, 0.0), axis=0, keepdims=True)


def dot_nt(a, b):
    return lax.dot_general(a, b, (((1,), (1,)), ((), ())), preferred_element_type=F32)


def flush_kernel(*refs):
    count = (len(refs) - 1) // 2
    copies = [
        pltpu.make_async_copy(refs[i], refs[count + i], refs[-1].at[i]) for i in range(count)
    ]
    for copy in copies:
        copy.start()
    for copy in copies:
        copy.wait()


def whole(ref, sem):
    return pltpu.make_async_copy(ref, ref, sem)


def flipped(me, k):
    peer, bit = me, 1
    while bit <= k:
        if k & bit:
            peer = peer + bit * (1 - 2 * ((me // bit) % 2))
        bit *= 2
    return peer


def feed_kernel(
    n_ep, n_tp, chunk, small, *refs,
):
    (
        tokens_hbm, wi_hbm, wf_hbm, bias_hbm, head_gain_hbm, mixer_gain_hbm, old_norm_hbm, old_max_hbm,
        feed_gain_hbm, blend_hbm, routes_hbm, scores_hbm,
    ) = refs[:small]
    (
        wq, wk, wv, wo, matrix_hbm, merge_hbm, gate_hbm, up_hbm, down_hbm, left_hbm, right_hbm, ddown_hbm,
        out, new_matrix, new_norm, new_max,
        wquery, wbuf, mbuf, spread, numer, aux, merge, gate_up, down, sides, ddown,
        head_send, head_recv, resid_buf, norm_buf, route_buf, route_all, route_far, every,
        hidden, part_send, part_recv, dense, ret_send, ret_recv,
        msem, wsem, head_sem, route_sem, ag_sem, ag_rsem, fwd_sem, part_sem, ret_sem,
    ) = refs[small : -small - 1]
    held, small_sems = refs[-small - 1 : -1], refs[-1]
    (
        tokens, wi, wf, bias, head_gain, mixer_gain, old_norm, old_max, feed_gain, blend_weight,
        routes, scores,
    ) = held

    small_copies = [
        pltpu.make_async_copy(refs[i], held[i], small_sems.at[i]) for i in range(small)
    ]
    wcopies = [
        pltpu.make_async_copy(ref, wbuf.at[i], wsem.at[0]) for i, ref in enumerate((wk, wv, wo))
    ]
    query_copy = pltpu.make_async_copy(wq, wquery, wsem.at[6])
    for copy in small_copies:
        copy.start()
    query_copy.start()

    me = lax.axis_index("ep")
    core = lax.axis_index("tp")
    partner = {"tp": 1 - core}
    rows, width = tokens.shape
    half = rows // n_tp
    hub = n_tp - 1
    side = n_ep // 2
    peers = {k: flipped(me, k) for k in range(1, n_ep)}
    upper = me // side
    near_peers = [peers[k] for k in range(side - 1, 0, -1)]
    far_peers = []
    for j in range(side // 2):
        pair = (1 - upper) * (side - 1 - j) + upper * j
        far_peers += [2 * pair + 1 - me % 2, 2 * pair + me % 2]
    near_first = (me // side) * side
    far_first = side - near_first

    barrier = pltpu.get_barrier_semaphore()
    pl.semaphore_signal(barrier, inc=1, device_id=partner, device_id_type=MESH)
    for peer in far_peers:
        pl.semaphore_signal(barrier, inc=1, device_id={"ep": peer, "tp": hub}, device_id_type=MESH)
    for peer in near_peers:
        pl.semaphore_signal(barrier, inc=1, device_id={"ep": peer, "tp": 0}, device_id_type=MESH)
    for copy in wcopies:
        copy.start()

    chunks = rows // chunk
    mcopies = [
        pltpu.make_async_copy(
            matrix_hbm.at[pl.ds(c * chunk, chunk)], mbuf.at[pl.ds(c * chunk, chunk)], msem.at[c]
        )
        for c in range(chunks)
    ]
    merge_copy = pltpu.make_async_copy(merge_hbm, merge, wsem.at[1])
    side_copies = [
        pltpu.make_async_copy(ref, sides.at[i], wsem.at[2]) for i, ref in enumerate((left_hbm, right_hbm))
    ]
    down_copy = pltpu.make_async_copy(down_hbm.at[0], down, wsem.at[3])
    ddown_copy = pltpu.make_async_copy(ddown_hbm, ddown, wsem.at[4])
    tiles = gate_up.shape[0]
    gu_copies = []
    for j in range(tiles):
        for column, ref in enumerate((gate_hbm, up_hbm)):
            gu_copies.append(
                pltpu.make_async_copy(
                    ref.at[0, :, pl.ds(j * LANES, LANES)],
                    gate_up.at[j, :, pl.ds(column * LANES, LANES)],
                    wsem.at[5],
                )
            )
    for copy in small_copies:
        copy.wait()
    for copy in mcopies + [merge_copy]:
        copy.start()

    heads, size = head_gain.shape
    inner = heads * size
    mixed = rms_rows(tokens[...].astype(F32), mixer_gain[...])
    mixed_f = mixed.astype(F32)
    keeps, writes, maxes = [], [], []
    for h in range(heads):
        in_gate = jnp.sum(mixed_f * wi[h : h + 1, :].astype(F32), axis=-1, keepdims=True)
        pre = jnp.sum(mixed_f * wf[h : h + 1, :].astype(F32), axis=-1, keepdims=True) + bias[:, h : h + 1]
        log_forget = jnp.minimum(pre, 0.0) - jnp.log1p(jnp.exp(-jnp.abs(pre)))
        old = to_column(old_max[h : h + 1, :])
        top = jnp.maximum(log_forget + old, in_gate)
        keeps.append(jnp.exp(log_forget + old - top))
        writes.append(jnp.exp(in_gate - top))
        maxes.append(top)

    query_copy.wait()
    query = jnp.dot(mixed, wquery[...], preferred_element_type=F32)
    high = query.astype(BF16)
    rest = query - high.astype(F32)
    middle = rest.astype(BF16)
    low = (rest - middle.astype(F32)).astype(BF16)
    terms = jnp.concatenate([high, middle, low], axis=0)
    lines = lax.broadcasted_iota(jnp.int32, (3 * rows, rows * size), 0)
    columns = lax.broadcasted_iota(jnp.int32, (3 * rows, rows * size), 1)
    pick = jnp.where(lax.rem(lines, rows) == columns // size, 1.0, 0.0).astype(BF16)
    spread[...] = lax.dot_general(
        terms, pick, (((0,), (0,)), ((), ())), preferred_element_type=F32
    )

    whole(wbuf, wsem.at[0]).wait()

    def project(i):
        return jnp.dot(mixed, wbuf[i], preferred_element_type=F32)

    keys = project(0) * size ** (-0.5)
    values = project(1)
    outgate = project(2)
    aux[:, :inner] = values
    denoms, crosses = [], []
    for h in range(heads):
        span = slice(h * size, (h + 1) * size)
        written = writes[h] * keys[:, span]
        aux[:, inner + h * size : inner + (h + 1) * size] = written
        fresh = keeps[h] * old_norm[:, h, :] + written
        new_norm[:, h, :] = fresh
        denoms.append(jnp.sum(query[:, span] * fresh, axis=-1, keepdims=True))
        crosses.append(jnp.sum(query[:, span] * written, axis=-1, keepdims=True))
    for c in range(chunks):
        mcopies[c].wait()
        for b in range(c * chunk, (c + 1) * chunk):
            for h in range(heads):
                numer[b : b + 1, h * size : (h + 1) * size] = jnp.sum(
                    spread[h * size : (h + 1) * size, b * size : (b + 1) * size] * mbuf[b, h],
                    axis=0,
                    keepdims=True,
                )
    energy = jnp.zeros((rows, 1), F32)
    gated = []
    for h in range(heads):
        span = slice(h * size, (h + 1) * size)
        readout = (keeps[h] * numer[:, span] + crosses[h] * values[:, span]) / jnp.maximum(
            jnp.abs(denoms[h]), jnp.exp(-maxes[h])
        )
        energy = energy + jnp.sum(readout * readout, axis=-1, keepdims=True)
        gated.append(
            (readout * head_gain[h : h + 1, :] * sigmoid(outgate[:, span])).astype(BF16)
        )
    merge_copy.wait()
    head_part = jnp.dot(
        jnp.concatenate(gated, axis=1), merge[...], preferred_element_type=F32
    )
    head_send[:, :width] = head_part
    head_send[:, width:] = jnp.broadcast_to(energy, (rows, LANES))

    @pl.when(core == hub)
    def _():
        pl.semaphore_wait(barrier, 2 * len(far_peers) + 1)

    @pl.when(core != hub)
    def _():
        pl.semaphore_wait(barrier, 2 * len(near_peers) + 1)

    head_copy = pltpu.make_async_remote_copy(
        head_send, head_recv, head_sem.at[0], head_sem.at[1], device_id=partner, device_id_type=MESH
    )
    head_copy.start()
    for copy in gu_copies + [down_copy]:
        copy.start()

    @pl.when(core == hub)
    def _():
        for copy in side_copies + [ddown_copy]:
            copy.start()

    def send(source, slot, send_sem, recv_sem, device):
        pltpu.make_async_remote_copy(
            source, slot, send_sem, recv_sem, device_id=device, device_id_type=MESH
        ).start()

    def all_others(slots, sem):
        return whole(slots.at[pl.ds(0, n_ep - 1)], sem)

    picks = routes.shape[0]
    score = scores[...].astype(F32)
    raised = jnp.exp(score - jnp.max(score, axis=0, keepdims=True))
    route_weight = raised / jnp.sum(raised, axis=0, keepdims=True)
    chosen = routes[...]
    route_buf[...] = jnp.zeros_like(route_buf)
    for e in range(n_ep):
        named = jnp.zeros((1, rows), F32)
        for p in range(picks):
            named = named + jnp.where(chosen[p : p + 1, :] == e, route_weight[p : p + 1, :], 0.0)
        route_buf[e, :, :rows] = named
    route_all[me] = route_buf[me]

    def spread_routes(targets):
        for peer in targets:
            send(
                route_buf.at[peer], route_all.at[me], route_sem.at[0], route_sem.at[1],
                {"ep": peer, "tp": hub},
            )

    @pl.when(core == hub)
    def _():
        spread_routes(far_peers)

    @pl.when(core != hub)
    def _():
        spread_routes(near_peers)

    for h in range(heads):
        new_max[h : h + 1, :] = to_row(maxes[h])

    head_copy.wait()
    head_total = head_part + head_recv[:, :width]
    energy_total = energy + head_recv[:, width : width + 1]
    scale = lax.rsqrt(energy_total / (inner * n_tp) + epsilon)
    resid = (tokens[...].astype(F32) + scale * head_total).astype(BF16).astype(F32)
    norm_buf[...] = rms_rows(resid, feed_gain[...])

    def spread_rows(targets):
        for peer in targets:
            send(norm_buf, every.at[me], ag_sem, ag_rsem.at[me], {"ep": peer, "tp": hub})

    @pl.when(core == hub)
    def _():
        spread_rows(far_peers)

    @pl.when(core != hub)
    def _():
        spread_rows(near_peers)

    every[me] = norm_buf[...]

    for i in range(n_tp):
        resid_buf[i] = resid[i * half : (i + 1) * half]

    for h in range(heads):
        key_cols = aux[:, inner + h * size : inner + (h + 1) * size].T
        for b in range(rows):
            new_matrix[b, h] = (
                keeps[h][b : b + 1, :] * mbuf[b, h]
                + key_cols[:, b : b + 1] * aux[b : b + 1, h * size : (h + 1) * size]
            )

    @pl.when(core == hub)
    def _():
        for i in range(n_ep - 1):
            origin = i + (i - me + n_ep) // n_ep
            whole(every.at[origin], ag_rsem.at[origin]).wait()
            send(every.at[origin], every.at[origin], fwd_sem.at[0], fwd_sem.at[1], partner)

    @pl.when(core != hub)
    def _():
        down_copy.wait()
        whole(gate_up, wsem.at[5]).wait()
        all_others(every, fwd_sem.at[1]).wait()

    count = n_ep * rows
    block = count // 2
    near_span = pl.ds(pl.multiple_of(near_first * rows, block), block)
    far_span = pl.ds(pl.multiple_of(far_first * rows, block), block)

    def fill_hidden():
        all_rows = every[...].reshape(count, width)
        for j in range(tiles):
            both = jnp.dot(all_rows, gate_up[j], preferred_element_type=F32)
            hidden[:, j * LANES : (j + 1) * LANES] = (
                silu(both[:, :LANES]) * both[:, LANES:]
            ).astype(BF16)

    def part_of(span):
        return jnp.dot(hidden[span, :], down[...], preferred_element_type=F32).astype(BF16)

    def weights_of(table, first):
        weights = jnp.broadcast_to(table[pl.ds(first, side)], (side, rows, LANES)).reshape(block, LANES)
        token = lax.rem(lax.broadcasted_iota(jnp.int32, (block, LANES), 0), rows)
        lane = lax.broadcasted_iota(jnp.int32, (block, LANES), 1)
        return jnp.sum(jnp.where(lane == token, weights, 0.0), axis=-1, keepdims=True)

    def give_back(combined, targets, first):
        ret_send[...] = combined.reshape(side, n_tp, half, width).astype(BF16)
        for peer in targets:
            for i in range(n_tp):
                send(
                    ret_send.at[peer - first, i], ret_recv.at[me], ret_sem.at[0], ret_sem.at[1],
                    {"ep": peer, "tp": i},
                )

    @pl.when(core != hub)
    def _():
        fill_hidden()
        part_send[...] = part_of(far_span)
        send(part_send, part_recv, part_sem.at[0], part_sem.at[1], partner)
        part = part_of(near_span).astype(F32)
        whole(route_far, route_sem.at[3]).wait()
        own_weight = weights_of(route_far, near_first)
        whole(part_recv, part_sem.at[1]).wait()
        give_back(own_weight * part + part_recv[...].astype(F32), near_peers, near_first)
        send(ret_send.at[me - near_first, hub], ret_recv.at[me], ret_sem.at[0], ret_sem.at[1], partner)
        ret_recv[me] = ret_send[me - near_first, 0]
        if near_peers:
            whole(route_all.at[pl.ds(0, side - 1)], route_sem.at[0]).wait()
            whole(every.at[pl.ds(0, side - 1)], ag_sem).wait()
        whole(part_send, part_sem.at[0]).wait()
        all_others(ret_recv, ret_sem.at[1]).wait()

    @pl.when(core == hub)
    def _():
        down_copy.wait()
        whole(gate_up, wsem.at[5]).wait()
        whole(sides, wsem.at[2]).wait()
        ddown_copy.wait()
        all_others(route_all, route_sem.at[1]).wait()
        send(route_all, route_far, route_sem.at[2], route_sem.at[3], partner)
        fill_hidden()
        near_part = part_of(near_span).astype(F32)
        inputs = every[...].reshape(count, width)
        blend = sigmoid(jnp.sum(inputs.astype(F32) * blend_weight[...], axis=-1, keepdims=True))
        dense_hidden = (silu(dot_nt(inputs, sides[0])) * dot_nt(inputs, sides[1])).astype(BF16)
        dense[...] = blend * jnp.dot(dense_hidden, ddown[...], preferred_element_type=F32)
        part_send[...] = (weights_of(route_all, near_first) * near_part + dense[near_span, :]).astype(BF16)
        send(part_send, part_recv, part_sem.at[0], part_sem.at[1], partner)
        part = part_of(far_span).astype(F32)
        own_weight = weights_of(route_all, far_first)
        whole(part_recv, part_sem.at[1]).wait()
        expert_out = (part + part_recv[...].astype(F32)).astype(BF16).astype(F32)
        give_back(own_weight * expert_out + dense[far_span, :], far_peers, far_first)
        whole(route_all.at[pl.ds(0, side)], route_sem.at[0]).wait()
        whole(route_all, route_sem.at[2]).wait()
        whole(every.at[pl.ds(0, side)], ag_sem).wait()
        all_others(every, fwd_sem.at[0]).wait()
        whole(part_send, part_sem.at[0]).wait()
        whole(ret_recv, ret_sem.at[1]).wait()

    total = resid_buf[core]
    for e in range(n_ep):
        total = total + ret_recv[e].astype(F32)
    out[...] = total.astype(BF16)

    @pl.when(core == hub)
    def _():
        whole(ret_recv, ret_sem.at[0]).wait()

    @pl.when(core != hub)
    def _():
        all_others(ret_recv, ret_sem.at[0]).wait()


VMEM = pl.BlockSpec(memory_space=pltpu.VMEM)
ANY = pl.BlockSpec(memory_space=pl.ANY)


def local(
    n_ep, n_tp, tokens, query_weight, key_weight, value_weight, outgate_weight, ingate_weight,
    forget_weight, forget_bias, head_gain, merge_weight, mixer_gain, feed_gain, memory_matrix,
    memory_norm, memory_max, routes, route_scores, expert_gate, expert_up, expert_down,
    dense_left, dense_right, dense_down, blend_weight,
):
    rows, width = tokens.shape
    heads, size = head_gain.shape
    half = rows // n_tp
    chunk = max(1, rows // 2)
    chunks = rows // chunk
    dma = pltpu.SemaphoreType.DMA
    inner = expert_gate.shape[2]
    tiles = inner // LANES
    dense_inner = dense_left.shape[1]
    count = n_ep * rows
    lanes = heads * size
    small = (
        tokens, ingate_weight.T, forget_weight.T, forget_bias.reshape(1, heads), head_gain,
        mixer_gain.reshape(1, width), memory_norm, memory_max.T, feed_gain.reshape(1, width),
        blend_weight.reshape(1, width), routes.T, route_scores.T,
    )
    operands = (
        *small, query_weight, key_weight, value_weight, outgate_weight, memory_matrix, merge_weight, expert_gate, expert_up,
        expert_down, dense_left.T, dense_right.T, dense_down,
    )
    layer_half, matrix, norm_vec, new_max = pl.pallas_call(
        functools.partial(feed_kernel, n_ep, n_tp, chunk, len(small)),
        out_shape=(
            pltpu.VMEM((half, width), BF16),
            pltpu.VMEM(memory_matrix.shape, F32),
            pltpu.VMEM(memory_norm.shape, F32),
            pltpu.VMEM((heads, rows), F32),
        ),
        in_specs=[ANY] * (len(small) + 12),
        out_specs=(VMEM,) * 4,
        scratch_shapes=[
            pltpu.VMEM((width, lanes), BF16),
            pltpu.VMEM((3, width, lanes), BF16),
            pltpu.VMEM(memory_matrix.shape, F32),
            pltpu.VMEM((lanes, rows * size), F32),
            pltpu.VMEM((rows, lanes), F32),
            pltpu.VMEM((rows, 2 * lanes), F32),
            pltpu.VMEM(merge_weight.shape, BF16),
            pltpu.VMEM((tiles, width, 2 * LANES), BF16),
            pltpu.VMEM((inner, width), BF16),
            pltpu.VMEM((2, dense_inner, width), BF16),
            pltpu.VMEM((dense_inner, width), BF16),
            pltpu.VMEM((rows, width + LANES), F32),
            pltpu.VMEM((rows, width + LANES), F32),
            pltpu.VMEM((n_tp, half, width), F32),
            pltpu.VMEM((rows, width), BF16),
            pltpu.VMEM((n_ep, 1, LANES), F32),
            pltpu.VMEM((n_ep, 1, LANES), F32),
            pltpu.VMEM((n_ep, 1, LANES), F32),
            pltpu.VMEM((n_ep, rows, width), BF16),
            pltpu.VMEM((count, inner), BF16),
            pltpu.VMEM((count // 2, width), BF16),
            pltpu.VMEM((count // 2, width), BF16),
            pltpu.VMEM((count, width), F32),
            pltpu.VMEM((n_ep // 2, n_tp, half, width), BF16),
            pltpu.VMEM((n_ep, half, width), BF16),
            dma((chunks,)),
            dma((7,)),
            dma((2,)),
            dma((4,)),
            dma,
            dma((n_ep,)),
            dma((2,)),
            dma((2,)),
            dma((2,)),
            *(pltpu.VMEM(a.shape, a.dtype) for a in small),
            dma((len(small),)),
        ],
        compiler_params=pltpu.CompilerParams(
            collective_id=0, has_side_effects=True, vmem_limit_bytes=48 << 20
        ),
        name="feed_forward",
    )(*(pltpu.with_memory_space_constraint(a, pltpu.HBM) for a in operands))
    held = (layer_half, matrix, norm_vec, new_max)
    layer_out, matrix, norm_vec, new_max = pl.pallas_call(
        flush_kernel,
        out_shape=tuple(jax.ShapeDtypeStruct(a.shape, a.dtype) for a in held),
        in_specs=[VMEM] * 4,
        out_specs=(ANY,) * 4,
        scratch_shapes=[dma((4,))],
        compiler_params=pltpu.CompilerParams(vmem_limit_bytes=8 << 20),
        name="write_out",
    )(*held)
    return (layer_out, matrix, norm_vec, new_max.T)


def solution(mesh):
    row = ("grp", "ep")
    in_specs = (
        P(row, None),
        P(None, "tp"),
        P(None, "tp"),
        P(None, "tp"),
        P(None, "tp"),
        P(None, "tp"),
        P(None, "tp"),
        P("tp"),
        P("tp", None),
        P("tp", None),
        P(),
        P(),
        P(row, "tp", None, None),
        P(row, "tp", None),
        P(row, "tp"),
        P(row, None),
        P(row, None),
        P("ep", None, "tp"),
        P("ep", None, "tp"),
        P("ep", "tp", None),
        P(None, "ep"),
        P(None, "ep"),
        P("ep", None),
        P(),
    )
    out_specs = (
        P(("grp", "ep", "tp"), None),
        P(row, "tp", None, None),
        P(row, "tp", None),
        P(row, "tp"),
    )
    body = functools.partial(local, mesh.shape["ep"], mesh.shape["tp"])
    return jax.shard_map(body, mesh=mesh, in_specs=in_specs, out_specs=out_specs, check_vma=False)
```

```python
import functools

import jax
import jax.numpy as jnp
from jax import lax
from jax.experimental import pallas as pl
from jax.experimental.pallas import tpu as pltpu
from jax.sharding import PartitionSpec as P

epsilon = 1e-06
F32 = jnp.float32
BF16 = jnp.bfloat16
MESH = pl.DeviceIdType.MESH
LANES = 128


def rms_rows(floats, gains):
    scaled = floats * lax.rsqrt(jnp.mean(floats * floats, axis=-1, keepdims=True) + epsilon)
    return (scaled * gains).astype(BF16)


def silu(x):
    return x / (1.0 + jnp.exp(-x))


def sigmoid(x):
    return 1.0 / (1.0 + jnp.exp(-x))


def eye_mask(n):
    return lax.broadcasted_iota(jnp.int32, (n, n), 0) == lax.broadcasted_iota(jnp.int32, (n, n), 1)


def to_column(row):
    return jnp.sum(jnp.where(eye_mask(row.shape[1]), row, 0.0), axis=1, keepdims=True)


def to_row(column):
    return jnp.sum(jnp.where(eye_mask(column.shape[0]), column, 0.0), axis=0, keepdims=True)


def dot_nt(a, b):
    return lax.dot_general(a, b, (((1,), (1,)), ((), ())), preferred_element_type=F32)


def flush_kernel(*refs):
    count = (len(refs) - 1) // 2
    copies = [
        pltpu.make_async_copy(refs[i], refs[count + i], refs[-1].at[i]) for i in range(count)
    ]
    for copy in copies:
        copy.start()
    for copy in copies:
        copy.wait()


def whole(ref, sem):
    return pltpu.make_async_copy(ref, ref, sem)


def flipped(me, k):
    peer, bit = me, 1
    while bit <= k:
        if k & bit:
            peer = peer + bit * (1 - 2 * ((me // bit) % 2))
        bit *= 2
    return peer


def feed_kernel(
    n_ep, n_tp, chunk, small, *refs,
):
    (
        tokens_hbm, wi_hbm, wf_hbm, bias_hbm, head_gain_hbm, mixer_gain_hbm, old_norm_hbm, old_max_hbm,
        feed_gain_hbm, blend_hbm, routes_hbm, scores_hbm,
    ) = refs[:small]
    (
        wq, wk, wv, wo, matrix_hbm, merge_hbm, gate_hbm, up_hbm, down_hbm, left_hbm, right_hbm, ddown_hbm,
        out, new_matrix, new_norm, new_max,
        wquery, wbuf, mbuf, spread, numer, aux, merge, gate_up, down, sides, ddown,
        head_send, head_recv, resid_buf, norm_buf, route_buf, route_all, route_far, every,
        hidden, part_send, part_recv, dense, ret_send, ret_recv,
        msem, wsem, head_sem, route_sem, ag_sem, ag_rsem, fwd_sem, part_sem, ret_sem,
    ) = refs[small : -small - 1]
    held, small_sems = refs[-small - 1 : -1], refs[-1]
    (
        tokens, wi, wf, bias, head_gain, mixer_gain, old_norm, old_max, feed_gain, blend_weight,
        routes, scores,
    ) = held

    small_copies = [
        pltpu.make_async_copy(refs[i], held[i], small_sems.at[i]) for i in range(small)
    ]
    wcopies = [
        pltpu.make_async_copy(ref, wbuf.at[i], wsem.at[0]) for i, ref in enumerate((wk, wv, wo))
    ]
    query_copy = pltpu.make_async_copy(wq, wquery, wsem.at[6])
    for copy in small_copies:
        copy.start()
    query_copy.start()

    me = lax.axis_index("ep")
    core = lax.axis_index("tp")
    partner = {"tp": 1 - core}
    rows, width = tokens.shape
    half = rows // n_tp
    hub = n_tp - 1
    side = n_ep // 2
    peers = {k: flipped(me, k) for k in range(1, n_ep)}
    upper = me // side
    near_peers = [peers[k] for k in range(side - 1, 0, -1)]
    far_peers = []
    for j in range(side // 2):
        pair = (1 - upper) * (side - 1 - j) + upper * j
        far_peers += [2 * pair + 1 - me % 2, 2 * pair + me % 2]
    near_first = (me // side) * side
    far_first = side - near_first

    barrier = pltpu.get_barrier_semaphore()
    pl.semaphore_signal(barrier, inc=1, device_id=partner, device_id_type=MESH)
    for peer in far_peers:
        pl.semaphore_signal(barrier, inc=1, device_id={"ep": peer, "tp": hub}, device_id_type=MESH)
    for peer in near_peers:
        pl.semaphore_signal(barrier, inc=1, device_id={"ep": peer, "tp": 0}, device_id_type=MESH)
    for copy in wcopies:
        copy.start()

    chunks = rows // chunk
    mcopies = [
        pltpu.make_async_copy(
            matrix_hbm.at[pl.ds(c * chunk, chunk)], mbuf.at[pl.ds(c * chunk, chunk)], msem.at[c]
        )
        for c in range(chunks)
    ]
    merge_copy = pltpu.make_async_copy(merge_hbm, merge, wsem.at[1])
    side_copies = [
        pltpu.make_async_copy(ref, sides.at[i], wsem.at[2]) for i, ref in enumerate((left_hbm, right_hbm))
    ]
    down_copy = pltpu.make_async_copy(down_hbm.at[0], down, wsem.at[3])
    ddown_copy = pltpu.make_async_copy(ddown_hbm, ddown, wsem.at[4])
    tiles = gate_up.shape[0]
    gu_copies = []
    for j in range(tiles):
        for column, ref in enumerate((gate_hbm, up_hbm)):
            gu_copies.append(
                pltpu.make_async_copy(
                    ref.at[0, :, pl.ds(j * LANES, LANES)],
                    gate_up.at[j, :, pl.ds(column * LANES, LANES)],
                    wsem.at[5],
                )
            )
    for copy in small_copies:
        copy.wait()
    for copy in mcopies + [merge_copy]:
        copy.start()

    heads, size = head_gain.shape
    inner = heads * size
    mixed = rms_rows(tokens[...].astype(F32), mixer_gain[...])
    mixed_f = mixed.astype(F32)
    keeps, writes, maxes = [], [], []
    for h in range(heads):
        in_gate = jnp.sum(mixed_f * wi[h : h + 1, :].astype(F32), axis=-1, keepdims=True)
        pre = jnp.sum(mixed_f * wf[h : h + 1, :].astype(F32), axis=-1, keepdims=True) + bias[:, h : h + 1]
        log_forget = jnp.minimum(pre, 0.0) - jnp.log1p(jnp.exp(-jnp.abs(pre)))
        old = to_column(old_max[h : h + 1, :])
        top = jnp.maximum(log_forget + old, in_gate)
        keeps.append(jnp.exp(log_forget + old - top))
        writes.append(jnp.exp(in_gate - top))
        maxes.append(top)

    query_copy.wait()
    query = jnp.dot(mixed, wquery[...], preferred_element_type=F32)
    high = query.astype(BF16)
    rest = query - high.astype(F32)
    middle = rest.astype(BF16)
    low = (rest - middle.astype(F32)).astype(BF16)
    terms = jnp.concatenate([high, middle, low], axis=0)
    lines = lax.broadcasted_iota(jnp.int32, (3 * rows, rows * size), 0)
    columns = lax.broadcasted_iota(jnp.int32, (3 * rows, rows * size), 1)
    pick = jnp.where(lax.rem(lines, rows) == columns // size, 1.0, 0.0).astype(BF16)
    spread[...] = lax.dot_general(
        terms, pick, (((0,), (0,)), ((), ())), preferred_element_type=F32
    )

    whole(wbuf, wsem.at[0]).wait()

    def project(i):
        return jnp.dot(mixed, wbuf[i], preferred_element_type=F32)

    keys = project(0) * size ** (-0.5)
    values = project(1)
    outgate = project(2)
    aux[:, :inner] = values
    denoms, crosses = [], []
    for h in range(heads):
        span = slice(h * size, (h + 1) * size)
        written = writes[h] * keys[:, span]
        aux[:, inner + h * size : inner + (h + 1) * size] = written
        fresh = keeps[h] * old_norm[:, h, :] + written
        new_norm[:, h, :] = fresh
        denoms.append(jnp.sum(query[:, span] * fresh, axis=-1, keepdims=True))
        crosses.append(jnp.sum(query[:, span] * written, axis=-1, keepdims=True))
    for c in range(chunks):
        mcopies[c].wait()
        for b in range(c * chunk, (c + 1) * chunk):
            for h in range(heads):
                numer[b : b + 1, h * size : (h + 1) * size] = jnp.sum(
                    spread[h * size : (h + 1) * size, b * size : (b + 1) * size] * mbuf[b, h],
                    axis=0,
                    keepdims=True,
                )
    energy = jnp.zeros((rows, 1), F32)
    gated = []
    for h in range(heads):
        span = slice(h * size, (h + 1) * size)
        readout = (keeps[h] * numer[:, span] + crosses[h] * values[:, span]) / jnp.maximum(
            jnp.abs(denoms[h]), jnp.exp(-maxes[h])
        )
        energy = energy + jnp.sum(readout * readout, axis=-1, keepdims=True)
        gated.append(
            (readout * head_gain[h : h + 1, :] * sigmoid(outgate[:, span])).astype(BF16)
        )
    merge_copy.wait()
    head_part = jnp.dot(
        jnp.concatenate(gated, axis=1), merge[...], preferred_element_type=F32
    )
    head_send[:, :width] = head_part
    head_send[:, width:] = jnp.broadcast_to(energy, (rows, LANES))

    @pl.when(core == hub)
    def _():
        pl.semaphore_wait(barrier, 2 * len(far_peers) + 1)

    @pl.when(core != hub)
    def _():
        pl.semaphore_wait(barrier, 2 * len(near_peers) + 1)

    head_copy = pltpu.make_async_remote_copy(
        head_send, head_recv, head_sem.at[0], head_sem.at[1], device_id=partner, device_id_type=MESH
    )
    head_copy.start()
    for copy in gu_copies + [down_copy]:
        copy.start()

    @pl.when(core == hub)
    def _():
        for copy in side_copies + [ddown_copy]:
            copy.start()

    def send(source, slot, send_sem, recv_sem, device):
        pltpu.make_async_remote_copy(
            source, slot, send_sem, recv_sem, device_id=device, device_id_type=MESH
        ).start()

    def all_others(slots, sem):
        return whole(slots.at[pl.ds(0, n_ep - 1)], sem)

    picks = routes.shape[0]
    score = scores[...].astype(F32)
    raised = jnp.exp(score - jnp.max(score, axis=0, keepdims=True))
    route_weight = raised / jnp.sum(raised, axis=0, keepdims=True)
    chosen = routes[...]
    route_buf[...] = jnp.zeros_like(route_buf)
    for e in range(n_ep):
        named = jnp.zeros((1, rows), F32)
        for p in range(picks):
            named = named + jnp.where(chosen[p : p + 1, :] == e, route_weight[p : p + 1, :], 0.0)
        route_buf[e, :, :rows] = named
    route_all[me] = route_buf[me]

    def spread_routes(targets):
        for peer in targets:
            send(
                route_buf.at[peer], route_all.at[me], route_sem.at[0], route_sem.at[1],
                {"ep": peer, "tp": hub},
            )

    @pl.when(core == hub)
    def _():
        spread_routes(far_peers)

    @pl.when(core != hub)
    def _():
        spread_routes(near_peers)

    for h in range(heads):
        new_max[h : h + 1, :] = to_row(maxes[h])

    head_copy.wait()
    head_total = head_part + head_recv[:, :width]
    energy_total = energy + head_recv[:, width : width + 1]
    scale = lax.rsqrt(energy_total / (inner * n_tp) + epsilon)
    resid = (tokens[...].astype(F32) + scale * head_total).astype(BF16).astype(F32)
    norm_buf[...] = rms_rows(resid, feed_gain[...])

    def spread_rows(targets):
        for peer in targets:
            send(norm_buf, every.at[me], ag_sem, ag_rsem.at[me], {"ep": peer, "tp": hub})

    @pl.when(core == hub)
    def _():
        spread_rows(far_peers)

    @pl.when(core != hub)
    def _():
        spread_rows(near_peers)

    every[me] = norm_buf[...]

    for i in range(n_tp):
        resid_buf[i] = resid[i * half : (i + 1) * half]

    for h in range(heads):
        key_cols = aux[:, inner + h * size : inner + (h + 1) * size].T
        for b in range(rows):
            new_matrix[b, h] = (
                keeps[h][b : b + 1, :] * mbuf[b, h]
                + key_cols[:, b : b + 1] * aux[b : b + 1, h * size : (h + 1) * size]
            )

    @pl.when(core == hub)
    def _():
        for i in range(n_ep - 1):
            origin = i + (i - me + n_ep) // n_ep
            whole(every.at[origin], ag_rsem.at[origin]).wait()
            send(every.at[origin], every.at[origin], fwd_sem.at[0], fwd_sem.at[1], partner)

    @pl.when(core != hub)
    def _():
        down_copy.wait()
        whole(gate_up, wsem.at[5]).wait()
        all_others(every, fwd_sem.at[1]).wait()

    count = n_ep * rows
    block = count // 2
    near_span = pl.ds(pl.multiple_of(near_first * rows, block), block)
    far_span = pl.ds(pl.multiple_of(far_first * rows, block), block)

    def fill_hidden():
        all_rows = every[...].reshape(count, width)
        for j in range(tiles):
            both = jnp.dot(all_rows, gate_up[j], preferred_element_type=F32)
            hidden[:, j * LANES : (j + 1) * LANES] = (
                silu(both[:, :LANES]) * both[:, LANES:]
            ).astype(BF16)

    def part_of(span):
        return jnp.dot(hidden[span, :], down[...], preferred_element_type=F32).astype(BF16)

    def weights_of(table, first):
        weights = jnp.broadcast_to(table[pl.ds(first, side)], (side, rows, LANES)).reshape(block, LANES)
        token = lax.rem(lax.broadcasted_iota(jnp.int32, (block, LANES), 0), rows)
        lane = lax.broadcasted_iota(jnp.int32, (block, LANES), 1)
        return jnp.sum(jnp.where(lane == token, weights, 0.0), axis=-1, keepdims=True)

    def give_back(combined, targets, first):
        ret_send[...] = combined.reshape(side, n_tp, half, width).astype(BF16)
        for peer in targets:
            for i in range(n_tp):
                send(
                    ret_send.at[peer - first, i], ret_recv.at[me], ret_sem.at[0], ret_sem.at[1],
                    {"ep": peer, "tp": i},
                )

    @pl.when(core != hub)
    def _():
        fill_hidden()
        part_send[...] = part_of(far_span)
        send(part_send, part_recv, part_sem.at[0], part_sem.at[1], partner)
        part = part_of(near_span).astype(F32)
        whole(route_far, route_sem.at[3]).wait()
        own_weight = weights_of(route_far, near_first)
        whole(part_recv, part_sem.at[1]).wait()
        give_back(own_weight * part + part_recv[...].astype(F32), near_peers, near_first)
        send(ret_send.at[me - near_first, hub], ret_recv.at[me], ret_sem.at[0], ret_sem.at[1], partner)
        ret_recv[me] = ret_send[me - near_first, 0]
        if near_peers:
            whole(route_all.at[pl.ds(0, side - 1)], route_sem.at[0]).wait()
            whole(every.at[pl.ds(0, side - 1)], ag_sem).wait()
        whole(part_send, part_sem.at[0]).wait()
        all_others(ret_recv, ret_sem.at[1]).wait()

    @pl.when(core == hub)
    def _():
        down_copy.wait()
        whole(gate_up, wsem.at[5]).wait()
        whole(sides, wsem.at[2]).wait()
        ddown_copy.wait()
        all_others(route_all, route_sem.at[1]).wait()
        send(route_all, route_far, route_sem.at[2], route_sem.at[3], partner)
        fill_hidden()
        near_part = part_of(near_span).astype(F32)
        part = part_of(far_span).astype(F32)
        inputs = every[...].reshape(count, width)
        blend = sigmoid(jnp.sum(inputs.astype(F32) * blend_weight[...], axis=-1, keepdims=True))
        dense_hidden = (silu(dot_nt(inputs, sides[0])) * dot_nt(inputs, sides[1])).astype(BF16)
        dense[...] = blend * jnp.dot(dense_hidden, ddown[...], preferred_element_type=F32)
        part_send[...] = (weights_of(route_all, near_first) * near_part + dense[near_span, :]).astype(BF16)
        send(part_send, part_recv, part_sem.at[0], part_sem.at[1], partner)
        own_weight = weights_of(route_all, far_first)
        whole(part_recv, part_sem.at[1]).wait()
        expert_out = (part + part_recv[...].astype(F32)).astype(BF16).astype(F32)
        give_back(own_weight * expert_out + dense[far_span, :], far_peers, far_first)
        whole(route_all.at[pl.ds(0, side)], route_sem.at[0]).wait()
        whole(route_all, route_sem.at[2]).wait()
        whole(every.at[pl.ds(0, side)], ag_sem).wait()
        all_others(every, fwd_sem.at[0]).wait()
        whole(part_send, part_sem.at[0]).wait()
        whole(ret_recv, ret_sem.at[1]).wait()

    total = resid_buf[core]
    for e in range(n_ep):
        total = total + ret_recv[e].astype(F32)
    out[...] = total.astype(BF16)

    @pl.when(core == hub)
    def _():
        whole(ret_recv, ret_sem.at[0]).wait()

    @pl.when(core != hub)
    def _():
        all_others(ret_recv, ret_sem.at[0]).wait()


VMEM = pl.BlockSpec(memory_space=pltpu.VMEM)
ANY = pl.BlockSpec(memory_space=pl.ANY)


def local(
    n_ep, n_tp, tokens, query_weight, key_weight, value_weight, outgate_weight, ingate_weight,
    forget_weight, forget_bias, head_gain, merge_weight, mixer_gain, feed_gain, memory_matrix,
    memory_norm, memory_max, routes, route_scores, expert_gate, expert_up, expert_down,
    dense_left, dense_right, dense_down, blend_weight,
):
    rows, width = tokens.shape
    heads, size = head_gain.shape
    half = rows // n_tp
    chunk = max(1, rows // 2)
    chunks = rows // chunk
    dma = pltpu.SemaphoreType.DMA
    inner = expert_gate.shape[2]
    tiles = inner // LANES
    dense_inner = dense_left.shape[1]
    count = n_ep * rows
    lanes = heads * size
    small = (
        tokens, ingate_weight.T, forget_weight.T, forget_bias.reshape(1, heads), head_gain,
        mixer_gain.reshape(1, width), memory_norm, memory_max.T, feed_gain.reshape(1, width),
        blend_weight.reshape(1, width), routes.T, route_scores.T,
    )
    operands = (
        *small, query_weight, key_weight, value_weight, outgate_weight, memory_matrix, merge_weight, expert_gate, expert_up,
        expert_down, dense_left.T, dense_right.T, dense_down,
    )
    layer_half, matrix, norm_vec, new_max = pl.pallas_call(
        functools.partial(feed_kernel, n_ep, n_tp, chunk, len(small)),
        out_shape=(
            pltpu.VMEM((half, width), BF16),
            pltpu.VMEM(memory_matrix.shape, F32),
            pltpu.VMEM(memory_norm.shape, F32),
            pltpu.VMEM((heads, rows), F32),
        ),
        in_specs=[ANY] * (len(small) + 12),
        out_specs=(VMEM,) * 4,
        scratch_shapes=[
            pltpu.VMEM((width, lanes), BF16),
            pltpu.VMEM((3, width, lanes), BF16),
            pltpu.VMEM(memory_matrix.shape, F32),
            pltpu.VMEM((lanes, rows * size), F32),
            pltpu.VMEM((rows, lanes), F32),
            pltpu.VMEM((rows, 2 * lanes), F32),
            pltpu.VMEM(merge_weight.shape, BF16),
            pltpu.VMEM((tiles, width, 2 * LANES), BF16),
            pltpu.VMEM((inner, width), BF16),
            pltpu.VMEM((2, dense_inner, width), BF16),
            pltpu.VMEM((dense_inner, width), BF16),
            pltpu.VMEM((rows, width + LANES), F32),
            pltpu.VMEM((rows, width + LANES), F32),
            pltpu.VMEM((n_tp, half, width), F32),
            pltpu.VMEM((rows, width), BF16),
            pltpu.VMEM((n_ep, 1, LANES), F32),
            pltpu.VMEM((n_ep, 1, LANES), F32),
            pltpu.VMEM((n_ep, 1, LANES), F32),
            pltpu.VMEM((n_ep, rows, width), BF16),
            pltpu.VMEM((count, inner), BF16),
            pltpu.VMEM((count // 2, width), BF16),
            pltpu.VMEM((count // 2, width), BF16),
            pltpu.VMEM((count, width), F32),
            pltpu.VMEM((n_ep // 2, n_tp, half, width), BF16),
            pltpu.VMEM((n_ep, half, width), BF16),
            dma((chunks,)),
            dma((7,)),
            dma((2,)),
            dma((4,)),
            dma,
            dma((n_ep,)),
            dma((2,)),
            dma((2,)),
            dma((2,)),
            *(pltpu.VMEM(a.shape, a.dtype) for a in small),
            dma((len(small),)),
        ],
        compiler_params=pltpu.CompilerParams(
            collective_id=0, has_side_effects=True, vmem_limit_bytes=48 << 20
        ),
        name="feed_forward",
    )(*(pltpu.with_memory_space_constraint(a, pltpu.HBM) for a in operands))
    held = (layer_half, matrix, norm_vec, new_max)
    layer_out, matrix, norm_vec, new_max = pl.pallas_call(
        flush_kernel,
        out_shape=tuple(jax.ShapeDtypeStruct(a.shape, a.dtype) for a in held),
        in_specs=[VMEM] * 4,
        out_specs=(ANY,) * 4,
        scratch_shapes=[dma((4,))],
        compiler_params=pltpu.CompilerParams(vmem_limit_bytes=8 << 20),
        name="write_out",
    )(*held)
    return (layer_out, matrix, norm_vec, new_max.T)


def solution(mesh):
    row = ("grp", "ep")
    in_specs = (
        P(row, None),
        P(None, "tp"),
        P(None, "tp"),
        P(None, "tp"),
        P(None, "tp"),
        P(None, "tp"),
        P(None, "tp"),
        P("tp"),
        P("tp", None),
        P("tp", None),
        P(),
        P(),
        P(row, "tp", None, None),
        P(row, "tp", None),
        P(row, "tp"),
        P(row, None),
        P(row, None),
        P("ep", None, "tp"),
        P("ep", None, "tp"),
        P("ep", "tp", None),
        P(None, "ep"),
        P(None, "ep"),
        P("ep", None),
        P(),
    )
    out_specs = (
        P(("grp", "ep", "tp"), None),
        P(row, "tp", None, None),
        P(row, "tp", None),
        P(row, "tp"),
    )
    body = functools.partial(local, mesh.shape["ep"], mesh.shape["tp"])
    return jax.shard_map(body, mesh=mesh, in_specs=in_specs, out_specs=out_specs, check_vma=False)
```
